256 devices in a mesh: sp: 16 (over y, x), tp: 16 (over z, core).
Axes of the slice: x: 4, y: 4, z: 8, core: 2. Of those that a mesh axis runs over, the one named last changes fastest.
Arguments:
- residual: bfloat16 [16384, 2048], P(('sp', 'tp')), may hold values from -6 to 6
- wide_query: bfloat16 [16384, 1024], P('sp', 'tp'), may hold values from -8 to 8
- narrow_query: bfloat16 [16384, 1024], P('sp', 'tp'), may hold values from -8 to 8
- wide_keys: bfloat16 [16384, 256], P('sp'), may hold values from -6 to 6
- narrow_keys: bfloat16 [16384, 256], P('sp'), may hold values from -6 to 6
- wide_values: bfloat16 [16384, 256], P('sp'), may hold values from -6 to 6
- narrow_values: bfloat16 [16384, 256], P('sp'), may hold values from -6 to 6
- wide_query_gain: float32 [64], replicated, may hold values from 1.2 to 10
- wide_key_gain: float32 [64], replicated, may hold values from 1.2 to 10
- narrow_query_gain: float32 [32], replicated, may hold values from 1.2 to 10
- narrow_key_gain: float32 [32], replicated, may hold values from 1.2 to 10
- wide_out: bfloat16 [1024, 2048], P('tp'), may hold values from -0.25 to 0.25
- narrow_out: bfloat16 [1024, 2048], P('tp'), may hold values from -0.25 to 0.25
- first_gain: float32 [2048], replicated, may hold values from 0.1 to 1.9
- first_bias: float32 [2048], replicated, may hold values from -1.8 to 1.8
- route_ids: int32 [16384, 2], P(('sp', 'tp')), may hold values from 0 to 31, all different within a row; in each aligned block of 64 rows (0 to 63, 64 to 127, ...) at most 5 rows name the same one
- route_weights: float32 [16384, 2], P(('sp', 'tp')), may hold values from 0.25 to 2.5
- expert_gate: bfloat16 [32, 2048, 3072], P('sp', None, 'tp'), may hold values from -0.125 to 0.125
- expert_up: bfloat16 [32, 2048, 3072], P('sp', None, 'tp'), may hold values from -0.125 to 0.125
- expert_down: bfloat16 [32, 3072, 2048], P('sp', 'tp'), may hold values from -0.109375 to 0.109375
- shared_gate: bfloat16 [2048, 256], replicated, may hold values from -0.125 to 0.125
- shared_up: bfloat16 [2048, 256], replicated, may hold values from -0.125 to 0.125
- shared_down: bfloat16 [256, 2048], replicated, may hold values from -0.375 to 0.375
- second_gain: float32 [2048], replicated, may hold values from 0.1 to 1.9
- second_bias: float32 [2048], replicated, may hold values from -1.8 to 1.8
Outputs:
- layer_output: bfloat16 [16384, 2048], P(('sp', 'tp'))
The draws below stay inside these ranges and needn't reach their ends.
Inputs may be any that keep to these rules, and one draw needn't show every extreme that they name: `route_ids`: each row names 2 different experts. The rows of one device (aligned blocks of 64 rows) name each expert at most 5 times, and in every draw some expert is named exactly 5 times in the rows of some device.
All inputs are finite; a program needn't handle non-finite values.
Results may differ from the reference program's by a relative error of at most 0.02.
The reference program's roundings to bfloat16 on the way count: a program that leaves them out, or rounds other values in their place, can miss the bound.
Values may be sent and summed in bfloat16 or wider, within the bound.
No kernel may reach another device: no remote copies, remote signals or barrier semaphores. Data moves between devices by JAX's collectives and lax.ppermute only.
A program may use at most 128 MiB of HBM per device.

```python
import math
import jax
import jax.numpy as jnp
import numpy as np
from jax import lax

MODEL_WIDTH = 2048
WIDE_HEADS = 16
WIDE_SIZE = 64
WIDE_GROUPS = 4
NARROW_HEADS = 32
NARROW_SIZE = 32
NARROW_GROUPS = 8
GRID_WIDTH = 64
EXPERT_WIDTH = 3072
SHARED_WIDTH = 256
ROUTE_TOP = 2
SEQ_TOKENS = 4096
TOKENS = 16384
DEVICE_ROWS = 64
EXPERTS = 32
CAPACITY = 5
N_SP = 16
N_TP = 16


def gain_pair(key, head_size, salt):
    folded = jax.random.fold_in(key, salt)
    draw_one = jax.random.uniform(jax.random.fold_in(folded, 2), (head_size,), jnp.float32)
    draw_two = jax.random.uniform(jax.random.fold_in(folded, 3), (head_size,), jnp.float32)
    query_gain = 1.5 * 2.0 ** draw_one
    key_gain = 1.5 * 2.0 ** draw_two
    return (query_gain, key_gain)


def field(key, heads, head_size, salt):
    folded = jax.random.fold_in(key, salt)
    return jnp.clip(jax.random.normal(folded, (TOKENS, heads, head_size), jnp.float32), -6.0, 6.0)


def drawn_queries(key, heads, head_size, salt):
    values = field(key, heads, head_size, salt + 100)
    return values.reshape(TOKENS, heads * head_size).astype(jnp.bfloat16)


def drawn_keys(key, heads, head_size, salt):
    values = field(key, heads, head_size, salt + 300)
    return values.reshape(TOKENS, heads * head_size).astype(jnp.bfloat16)


def draw_wide_query(key, part):
    return drawn_queries(key, WIDE_HEADS, WIDE_SIZE, 11)


def draw_narrow_query(key, part):
    return drawn_queries(key, NARROW_HEADS, NARROW_SIZE, 23)


def draw_wide_keys(key, part):
    return drawn_keys(key, WIDE_GROUPS, WIDE_SIZE, 11)


def draw_narrow_keys(key, part):
    return drawn_keys(key, NARROW_GROUPS, NARROW_SIZE, 23)


def draw_wide_query_gain(key, part):
    return gain_pair(key, WIDE_SIZE, 11)[0]


def draw_wide_key_gain(key, part):
    return gain_pair(key, WIDE_SIZE, 11)[1]


def draw_narrow_query_gain(key, part):
    return gain_pair(key, NARROW_SIZE, 23)[0]


def draw_narrow_key_gain(key, part):
    return gain_pair(key, NARROW_SIZE, 23)[1]


def levels(own_key, extent, shards, smallest, top_value):
    factor_of, own = 1.0, jax.random.fold_in(own_key, 6)
    for dim, parts in shards:
        heights = jnp.exp(jax.random.uniform(jax.random.fold_in(own, dim), (parts,), jnp.float32, smallest / len(shards), top_value / len(shards)))
        factor_of = factor_of * jnp.repeat(heights, extent[dim] // parts).reshape([-1 if axis == dim else 1 for axis in range(len(extent))])
    return factor_of


def shared_out(own_key, own, number, rows, number_of, top, bound, slope):
    ranking = jax.random.permutation(own_key, number_of)
    packed, usual = shares(number_of, rows * top, bound, slope, True), shares(number_of, rows * top, bound, slope, False)
    places = jnp.arange(number_of)

    def named(sizes, rotation):
        used = int((sizes > 0).sum())
        fixed = max(1, used // 4)
        passed = fixed + (places - fixed + rotation * (used - fixed)) % max(1, number_of - fixed)
        return jnp.zeros((number_of,), jnp.int32).at[ranking[jnp.where(places < fixed, places, passed)]].set(jnp.asarray(sizes, jnp.int32))

    sizes = jnp.where(number % 4 == 0, named(packed, number // 4), named(usual, number - number // 4 - 1))
    mixed = jax.random.permutation(jax.random.fold_in(own, 3), number_of)
    giver, sink = mixed[0:number_of // 2 * 2:2], mixed[1:number_of // 2 * 2:2]
    room = jnp.minimum(sizes[giver] - 1, bound - sizes[sink]) // 2
    room = jnp.where((giver == ranking[0]) | (sink == ranking[0]) | (sizes[sink] == 0), 0, jnp.maximum(room, 0))
    passed = jax.random.randint(jax.random.fold_in(own, 4), (number_of // 2,), 0, 1 << 20) % (room + 1)
    sizes = sizes.at[giver].add(-passed).at[sink].add(passed)
    items = jnp.searchsorted(jnp.cumsum(sizes), jnp.arange(rows * top), side="right").astype(jnp.int32)
    table = items.reshape(top, rows).T
    table = table[jax.random.permutation(jax.random.fold_in(own, 1), rows)]
    rotation = jax.random.randint(jax.random.fold_in(own, 2), (rows, 1), 0, top)
    return jnp.take_along_axis(table, (jnp.arange(top)[None, :] + rotation) % top, axis=1)


def shares(number_of, total, most, lean, full):
    weights = [(1 << 20) // math.isqrt(rank ** lean) + 1 for rank in range(1, number_of + 1)]
    largest = most if full else min(most, max(-(-total // number_of), total * weights[0] // sum(weights)))
    least = 1 if total - largest >= number_of - 1 else 0
    given, surplus = [largest] + [least] * (number_of - 1), total - largest - least * (number_of - 1)
    while surplus > 0:
        movable = [i for i in range(1, number_of) if given[i] < largest] or [i for i in range(1, number_of) if given[i] < most]
        pool, left = sum([weights[i] for i in movable]), surplus
        for i in movable:
            more = min(most - given[i], max(1, left * weights[i] // pool), surplus)
            given[i] = given[i] + more
            surplus = surplus - more
    return np.array(given)


def gaussian(rng, shape, scale, limit, cuts=(), kind=jnp.bfloat16):
    values = jax.random.normal(rng, shape, jnp.float32) * scale
    if len(cuts) > 0:
        values = levels(rng, shape, cuts, -0.22, 0.18) * values
    return jnp.clip(values, min=-limit, max=limit).astype(kind)


def setup_inputs(seed: int = 0) -> dict:
    streams_of = jax.random.split(jax.random.key(seed), 26)
    residual = gaussian(streams_of[0], (TOKENS, MODEL_WIDTH), 1.0, 6.0, ((0, 256),))
    wide_query = draw_wide_query(jax.random.fold_in(streams_of[25], 71), 0)
    narrow_query = draw_narrow_query(jax.random.fold_in(streams_of[25], 71), 0)
    wide_keys = draw_wide_keys(jax.random.fold_in(streams_of[25], 71), 0)
    narrow_keys = draw_narrow_keys(jax.random.fold_in(streams_of[25], 71), 0)
    wide_values = gaussian(streams_of[5], (TOKENS, WIDE_GROUPS * WIDE_SIZE), 1.0, 6.0, ((0, 16),))
    narrow_values = gaussian(streams_of[6], (TOKENS, NARROW_GROUPS * NARROW_SIZE), 1.0, 6.0, ((0, 16),))
    wide_query_gain = draw_wide_query_gain(jax.random.fold_in(streams_of[25], 71), 0)
    wide_key_gain = draw_wide_key_gain(jax.random.fold_in(streams_of[25], 71), 0)
    narrow_query_gain = draw_narrow_query_gain(jax.random.fold_in(streams_of[25], 71), 0)
    narrow_key_gain = draw_narrow_key_gain(jax.random.fold_in(streams_of[25], 71), 0)
    wide_out = gaussian(streams_of[11], (WIDE_HEADS * WIDE_SIZE, MODEL_WIDTH), (WIDE_HEADS * WIDE_SIZE // 2) ** -0.5, 0.25, ((0, 16),))
    narrow_out = gaussian(streams_of[12], (NARROW_HEADS * NARROW_SIZE, MODEL_WIDTH), (NARROW_HEADS * NARROW_SIZE // 2) ** -0.5, 0.25, ((0, 16),))
    first_gain = jnp.clip(1.0 + 0.18 * jax.random.normal(streams_of[13], (MODEL_WIDTH,), jnp.float32), 0.1, 1.9)
    first_bias = gaussian(streams_of[14], (MODEL_WIDTH,), 0.3, 1.8, (), jnp.float32)
    route_ids_keys = jax.random.split(jax.random.fold_in(streams_of[15], 1), TOKENS // DEVICE_ROWS)
    route_ids_turns = jax.random.permutation(jax.random.fold_in(streams_of[15], 3), TOKENS // DEVICE_ROWS)
    route_ids = jax.vmap(lambda own, number: shared_out(jax.random.fold_in(streams_of[15], 2), own, number, DEVICE_ROWS, EXPERTS, ROUTE_TOP, CAPACITY, 2))(route_ids_keys, route_ids_turns).reshape((TOKENS, ROUTE_TOP))
    route_weights = jnp.clip(jnp.exp(math.log(2.5) - 2.3025851 * jax.random.uniform(streams_of[16], (TOKENS, ROUTE_TOP), jnp.float32) ** levels(streams_of[16], (TOKENS, ROUTE_TOP), ((0, 256),), -0.2, 0.2)), 0.25, 2.5)
    expert_gate = gaussian(streams_of[17], (EXPERTS, MODEL_WIDTH, EXPERT_WIDTH), MODEL_WIDTH ** -0.5, 0.125, ((0, 16), (2, 16)))
    expert_up = gaussian(streams_of[18], (EXPERTS, MODEL_WIDTH, EXPERT_WIDTH), MODEL_WIDTH ** -0.5, 0.125, ((0, 16), (2, 16)))
    expert_down = gaussian(streams_of[19], (EXPERTS, EXPERT_WIDTH, MODEL_WIDTH), EXPERT_WIDTH ** -0.5, 0.109375, ((0, 16), (1, 16)))
    shared_gate = gaussian(streams_of[20], (MODEL_WIDTH, SHARED_WIDTH), MODEL_WIDTH ** -0.5, 0.125)
    shared_up = gaussian(streams_of[21], (MODEL_WIDTH, SHARED_WIDTH), MODEL_WIDTH ** -0.5, 0.125)
    shared_down = gaussian(streams_of[22], (SHARED_WIDTH, MODEL_WIDTH), SHARED_WIDTH ** -0.5, 0.375)
    second_gain = jnp.clip(1.0 + 0.18 * jax.random.normal(streams_of[23], (MODEL_WIDTH,), jnp.float32), 0.1, 1.9)
    second_bias = gaussian(streams_of[24], (MODEL_WIDTH,), 0.3, 1.8, (), jnp.float32)
    return {"residual": residual, "wide_query": wide_query, "narrow_query": narrow_query, "wide_keys": wide_keys, "narrow_keys": narrow_keys, "wide_values": wide_values, "narrow_values": narrow_values, "wide_query_gain": wide_query_gain, "wide_key_gain": wide_key_gain, "narrow_query_gain": narrow_query_gain, "narrow_key_gain": narrow_key_gain, "wide_out": wide_out, "narrow_out": narrow_out, "first_gain": first_gain, "first_bias": first_bias, "route_ids": route_ids, "route_weights": route_weights, "expert_gate": expert_gate, "expert_up": expert_up, "expert_down": expert_down, "shared_gate": shared_gate, "shared_up": shared_up, "shared_down": shared_down, "second_gain": second_gain, "second_bias": second_bias}


EPS_HEAD = 1e-06
EPS_LAYER = 1e-05
ALPHA = 2.0 ** 0.25
THETA = 10000.0

def head_norm(values, gain_vec):
    mean_square = lax.optimization_barrier(jnp.mean(values * values, axis=-1, keepdims=True))
    return values * lax.rsqrt(mean_square + EPS_HEAD) * gain_vec

def rotate(values, position):
    half_size = values.shape[-1] // 2
    frequency = THETA ** (-jnp.arange(half_size, dtype=jnp.float32) / half_size)
    angles = position.astype(jnp.float32)[:, None] * frequency
    cosine = jnp.cos(angles)[:, None, :]
    sine_part = jnp.sin(angles)[:, None, :]
    leading = values[..., :half_size]
    trailing = values[..., half_size:]
    return jnp.concatenate([leading * cosine - trailing * sine_part, trailing * cosine + leading * sine_part], axis=-1)

def grid_rotate(values, position):
    half_size = values.shape[-1] // 2
    grid_row = position // GRID_WIDTH
    grid_col = position % GRID_WIDTH
    return jnp.concatenate([rotate(values[..., :half_size], grid_row), rotate(values[..., half_size:], grid_col)], axis=-1)

def layer_norm(values, gain_vec, bias_vec):
    center = lax.optimization_barrier(jnp.mean(values, axis=-1, keepdims=True))
    shifted = values - center
    variance = lax.optimization_barrier(jnp.mean(shifted * shifted, axis=-1, keepdims=True))
    return (shifted * lax.rsqrt(variance + EPS_LAYER) * gain_vec + bias_vec).astype(jnp.bfloat16)

def attend_group(queries, keys_all, values_all, query_gain, key_gain, heads_total, groups):
    head_size = query_gain.shape[0]
    per_group = heads_total // groups
    seq_count = TOKENS // SEQ_TOKENS
    block_rows = min(512, SEQ_TOKENS)
    position = jnp.arange(SEQ_TOKENS, dtype=jnp.int32)
    score_scale = head_size ** (-0.5)
    query_seq = queries.reshape(seq_count, SEQ_TOKENS, heads_total, head_size)
    key_seq = keys_all.reshape(seq_count, SEQ_TOKENS, groups, head_size)
    value_seq = values_all.reshape(seq_count, SEQ_TOKENS, groups, head_size)

    def one_sequence(operands):
        query_rows, key_rows, value_rows = operands
        rotated_queries = grid_rotate(head_norm(query_rows.astype(jnp.float32), query_gain), position).astype(jnp.bfloat16)
        rotated_keys = grid_rotate(head_norm(key_rows.astype(jnp.float32), key_gain), position).astype(jnp.bfloat16)
        key_float = rotated_keys.astype(jnp.float32)
        value_float = value_rows.astype(jnp.float32)
        blocks = rotated_queries.reshape(SEQ_TOKENS // block_rows, block_rows, groups, per_group, head_size)

        def one_block(query_block):
            scores = jnp.einsum('qgpd,kgd->gpqk', query_block.astype(jnp.float32), key_float) * score_scale
            largest = lax.optimization_barrier(jnp.max(scores, axis=-1, keepdims=True))
            weights = jnp.exp(scores - largest)
            weights = (weights / lax.optimization_barrier(jnp.sum(weights, axis=-1, keepdims=True))).astype(jnp.bfloat16)
            mixed_rows = jnp.einsum('gpqk,kgd->qgpd', weights.astype(jnp.float32), value_float)
            return mixed_rows.astype(jnp.bfloat16)
        mixed_all = lax.map(one_block, blocks)
        return mixed_all.reshape(SEQ_TOKENS, heads_total * head_size)
    result = lax.map(one_sequence, (query_seq, key_seq, value_seq))
    return result.reshape(TOKENS, heads_total * head_size)

def routed_sum(hidden, route_ids, route_weights, expert_gate, expert_up, expert_down):
    assignments = TOKENS * ROUTE_TOP
    most = N_SP * N_TP * CAPACITY
    flat_ids = route_ids.reshape(-1).astype(jnp.int32)
    order = jnp.argsort(flat_ids, stable=True).astype(jnp.int32)
    counts = lax.optimization_barrier(jnp.sum((flat_ids[:, None] == jnp.arange(EXPERTS, dtype=jnp.int32)[None, :]).astype(jnp.int32), axis=0))
    starts = jnp.cumsum(counts) - counts
    slot_rank = jnp.arange(most, dtype=jnp.int32)
    position_in = (starts[:, None] + slot_rank[None, :]).astype(jnp.int32)
    valid = slot_rank[None, :] < counts[:, None]
    picked = jnp.where(valid, order[jnp.minimum(position_in, assignments - 1)], assignments).astype(jnp.int32)
    token_rows = (picked // ROUTE_TOP).astype(jnp.int32)
    padded_hidden = jnp.concatenate([hidden, jnp.zeros((1, MODEL_WIDTH), jnp.bfloat16)], axis=0)
    block_width = EXPERT_WIDTH // N_TP

    def one_expert(operands):
        rows_index, gate_weight, up_weight, down_weight = operands
        rows_in = padded_hidden[rows_index]
        gate_values = jnp.dot(rows_in, gate_weight, preferred_element_type=jnp.float32)
        up_values = jnp.dot(rows_in, up_weight, preferred_element_type=jnp.float32)
        active = (jax.nn.silu(gate_values) * up_values).astype(jnp.bfloat16)
        blocks_in = active.reshape(most, N_TP, block_width).astype(jnp.float32)
        down_blocks = down_weight.reshape(N_TP, block_width, MODEL_WIDTH).astype(jnp.float32)
        partial_value = lax.optimization_barrier(jnp.einsum('mtf,tfd->tmd', blocks_in, down_blocks).astype(jnp.bfloat16))
        return lax.optimization_barrier(jnp.sum(partial_value.astype(jnp.float32), axis=0)).astype(jnp.bfloat16)
    outputs = lax.map(one_expert, (token_rows, expert_gate, expert_up, expert_down))
    padded_weights = jnp.concatenate([route_weights.reshape(-1), jnp.zeros((1,), jnp.float32)], axis=0)
    slot_weight = padded_weights[picked]
    contribution = slot_weight[:, :, None] * outputs.astype(jnp.float32)
    total = jnp.zeros((TOKENS + 1, MODEL_WIDTH), jnp.float32).at[token_rows.reshape(-1)].add(contribution.reshape(-1, MODEL_WIDTH))
    return total[:TOKENS]

def reference(residual, wide_query, narrow_query, wide_keys, narrow_keys, wide_values, narrow_values, wide_query_gain, wide_key_gain, narrow_query_gain, narrow_key_gain, wide_out, narrow_out, first_gain, first_bias, route_ids, route_weights, expert_gate, expert_up, expert_down, shared_gate, shared_up, shared_down, second_gain, second_bias):
    wide_mixed = attend_group(wide_query, wide_keys, wide_values, wide_query_gain, wide_key_gain, WIDE_HEADS, WIDE_GROUPS)
    narrow_mixed = attend_group(narrow_query, narrow_keys, narrow_values, narrow_query_gain, narrow_key_gain, NARROW_HEADS, NARROW_GROUPS)
    projected = jnp.dot(wide_mixed, wide_out, preferred_element_type=jnp.float32) + jnp.dot(narrow_mixed, narrow_out, preferred_element_type=jnp.float32)
    hidden = layer_norm(ALPHA * residual.astype(jnp.float32) + projected, first_gain, first_bias)
    routed = routed_sum(hidden, route_ids, route_weights, expert_gate, expert_up, expert_down)
    shared_gate_values = jnp.dot(hidden, shared_gate, preferred_element_type=jnp.float32)
    shared_up_values = jnp.dot(hidden, shared_up, preferred_element_type=jnp.float32)
    shared_active = (jax.nn.silu(shared_gate_values) * shared_up_values).astype(jnp.bfloat16)
    shared_output = jnp.dot(shared_active, shared_down, preferred_element_type=jnp.float32)
    return layer_norm(ALPHA * hidden.astype(jnp.float32) + routed + shared_output, second_gain, second_bias)
```

```python
import jax
import jax.numpy as jnp
from jax import lax
from jax.experimental import pallas as pl
from jax.experimental.pallas import tpu as pltpu
from jax.sharding import PartitionSpec as P

LOCAL_EXPERTS = 2
EPS_LAYER = 1e-05
ALPHA = 2.0**0.25
EPS_HEAD = 1e-06
THETA = 10000.0
GRID_WIDTH = 64
SEQ_SHARDS = 4
LOG2E = 1.4426950408889634
WIDE_SIZE = 64
NARROW_SIZE = 32
KEY_ROWS = WIDE_SIZE + NARROW_SIZE
ONES_ROWS = 16
BLOCK_Q = 256
CHUNK = 512


def column(ref):
    size = ref.shape[1]
    spread = jnp.broadcast_to(ref[...], (size, size))
    diagonal = lax.broadcasted_iota(jnp.int32, (size, size), 0) == lax.broadcasted_iota(
        jnp.int32, (size, size), 1
    )
    return jnp.sum(jnp.where(diagonal, spread, 0.0), axis=1, keepdims=True)


def normed(heads, gain):
    mean_square = jnp.mean(heads * heads, axis=0, keepdims=True)
    return heads * lax.rsqrt(mean_square + EPS_HEAD) * gain


def turned(heads, tables):
    n = heads.shape[0] // 4
    parts = []
    for half, (cosine, sine) in enumerate(tables):
        a = heads[2 * half * n : (2 * half + 1) * n]
        b = heads[(2 * half + 1) * n : (2 * half + 2) * n]
        parts += [a * cosine - b * sine, b * cosine + a * sine]
    return jnp.concatenate(parts, axis=0)


def angle_tables(quarter, first_row, tokens):
    frequency = jnp.exp(
        lax.broadcasted_iota(jnp.int32, (quarter, tokens), 0).astype(jnp.float32)
        * (-jnp.log(jnp.float32(THETA)) / quarter)
    )
    token = lax.broadcasted_iota(jnp.int32, (quarter, tokens), 1)
    row_angle = (token // GRID_WIDTH + first_row).astype(jnp.float32) * frequency
    col_angle = (token % GRID_WIDTH).astype(jnp.float32) * frequency
    return ((jnp.cos(row_angle), jnp.sin(row_angle)), (jnp.cos(col_angle), jnp.sin(col_angle)))


def prepare_kernel(place, wqt, nqt, wk, nk, wv, nv, wqg, wkg, nqg, nkg, q_out, kv_out, turn):
    tokens = wqt.shape[1]
    tp = place[0]
    first_row = place[1]
    wide_tables = angle_tables(WIDE_SIZE // 4, first_row, tokens)
    narrow_tables = angle_tables(NARROW_SIZE // 4, first_row, tokens)

    def picked(ref, start, size):
        block = start // 128
        columns = ref[:, pl.ds(pl.multiple_of(block * 128, 128), 128)]
        turn[...] = columns.astype(jnp.float32).T
        return turn[pl.ds(pl.multiple_of(start % 128, size), size), :]

    wide_start = tp // 4 * WIDE_SIZE
    narrow_start = tp // 2 * NARROW_SIZE
    keys = turned(normed(picked(wk, wide_start, WIDE_SIZE), column(wkg)), wide_tables)
    kv_out[0:64, :] = keys.astype(jnp.bfloat16)
    keys = turned(normed(picked(nk, narrow_start, NARROW_SIZE), column(nkg)), narrow_tables)
    kv_out[64:96, :] = keys.astype(jnp.bfloat16)
    kv_out[96:160, :] = picked(wv, wide_start, WIDE_SIZE).astype(jnp.bfloat16)
    kv_out[160:192, :] = picked(nv, narrow_start, NARROW_SIZE).astype(jnp.bfloat16)
    wide = turned(normed(wqt[...].astype(jnp.float32), column(wqg)), wide_tables)
    q_out[0:64, 0:tokens] = wide.astype(jnp.bfloat16)
    q_out[64:128, 0:tokens] = jnp.zeros((64, tokens), jnp.bfloat16)
    q_out[0:64, tokens:] = jnp.zeros((64, 2 * tokens), jnp.bfloat16)
    q_out[96:128, tokens:] = jnp.zeros((32, 2 * tokens), jnp.bfloat16)
    for head in range(2):
        rows = nqt[NARROW_SIZE * head : NARROW_SIZE * (head + 1), :].astype(jnp.float32)
        narrow = turned(normed(rows, column(nqg)), narrow_tables)
        q_out[64:96, tokens * (head + 1) : tokens * (head + 2)] = narrow.astype(jnp.bfloat16)


def prepare(place, wqt, nqt, wk, nk, wv, nv, wqg, wkg, nqg, nkg):
    tokens = wqt.shape[1]
    vmem = pl.BlockSpec(memory_space=pltpu.VMEM)
    return pl.pallas_call(
        prepare_kernel,
        out_shape=(
            jax.ShapeDtypeStruct((128, 3 * tokens), jnp.bfloat16),
            jax.ShapeDtypeStruct((192, tokens), jnp.bfloat16),
        ),
        in_specs=[pl.BlockSpec(memory_space=pltpu.SMEM)] + [vmem] * 10,
        out_specs=(vmem, vmem),
        scratch_shapes=[pltpu.VMEM((128, tokens), jnp.float32)],
        name="prepare_heads",
    )(
        place, wqt, nqt, wk, nk, wv, nv,
        wqg.reshape(1, -1), wkg.reshape(1, -1), nqg.reshape(1, -1), nkg.reshape(1, -1),
    )


def attend_kernel(q, kv0, kv1, kv2, kv3, out, keys, values, scores0, scores1, mixed):
    tokens = kv0.shape[1]
    total = 4 * tokens
    blocks = q.shape[1] // BLOCK_Q
    wide_blocks = tokens // BLOCK_Q
    values[KEY_ROWS:, :] = jnp.ones((ONES_ROWS, total), jnp.bfloat16)
    for n, kv in enumerate((kv0, kv1, kv2, kv3)):
        piece = kv[0:KEY_ROWS, :].astype(jnp.float32)
        padded = jnp.concatenate([piece, jnp.zeros((128 - KEY_ROWS, tokens), jnp.float32)], axis=0)
        keys[n * tokens : (n + 1) * tokens, :] = padded.T.astype(jnp.bfloat16)
        values[0:KEY_ROWS, n * tokens : (n + 1) * tokens] = kv[KEY_ROWS:, :]

    def scored(c, query, into, largest):
        part = jnp.dot(
            keys[c * CHUNK : (c + 1) * CHUNK, :], query, preferred_element_type=jnp.float32
        )
        into[c * CHUNK : (c + 1) * CHUNK, :] = part
        return jnp.maximum(largest, jnp.max(part.reshape(CHUNK // 8, 8, BLOCK_Q), axis=0))

    lowest = jnp.full((8, BLOCK_Q), -jnp.inf, jnp.float32)
    query_at = lambda b: q[:, pl.ds(pl.multiple_of(b * BLOCK_Q, BLOCK_Q), BLOCK_Q)]

    def step(b, current, following, largest):
        query = query_at(jnp.minimum(b + 1, blocks - 1))
        peak = jnp.max(largest, axis=0, keepdims=True)
        factor = jnp.where(
            b < wide_blocks,
            jnp.float32(WIDE_SIZE**-0.5 * LOG2E),
            jnp.float32(NARROW_SIZE**-0.5 * LOG2E),
        )
        next_largest = lowest
        total_mixed = jnp.zeros((KEY_ROWS + ONES_ROWS, BLOCK_Q), jnp.float32)
        for c in range(total // CHUNK):
            next_largest = scored(c, query, following, next_largest)
            raw = current[c * CHUNK : (c + 1) * CHUNK, :]
            weights = jnp.exp2((raw - peak) * factor).astype(jnp.bfloat16)
            total_mixed = total_mixed + jnp.dot(
                values[:, c * CHUNK : (c + 1) * CHUNK], weights, preferred_element_type=jnp.float32
            )
        mixed[b] = total_mixed[:KEY_ROWS] / total_mixed[KEY_ROWS : KEY_ROWS + 1]
        return next_largest

    largest = lowest
    first = query_at(0)
    for c in range(total // CHUNK):
        largest = scored(c, first, scores0, largest)

    def pair(i, largest):
        largest = step(2 * i, scores0, scores1, largest)
        return step(2 * i + 1, scores1, scores0, largest)

    lax.fori_loop(0, blocks // 2, pair, largest)
    for b in range(wide_blocks):
        rows = jnp.concatenate(
            [
                mixed[b, 0:WIDE_SIZE],
                mixed[wide_blocks + b, WIDE_SIZE:KEY_ROWS],
                mixed[2 * wide_blocks + b, WIDE_SIZE:KEY_ROWS],
            ],
            axis=0,
        )
        out[b * BLOCK_Q : (b + 1) * BLOCK_Q, :] = rows.T.astype(jnp.bfloat16)


def attend(q, pieces):
    tokens = pieces[0].shape[1]
    vmem = pl.BlockSpec(memory_space=pltpu.VMEM)
    return pl.pallas_call(
        attend_kernel,
        out_shape=jax.ShapeDtypeStruct((tokens, 128), jnp.bfloat16),
        in_specs=[vmem] * 5,
        out_specs=vmem,
        scratch_shapes=[
            pltpu.VMEM((4 * tokens, 128), jnp.bfloat16),
            pltpu.VMEM((KEY_ROWS + ONES_ROWS, 4 * tokens), jnp.bfloat16),
            pltpu.VMEM((4 * tokens, BLOCK_Q), jnp.float32),
            pltpu.VMEM((4 * tokens, BLOCK_Q), jnp.float32),
            pltpu.VMEM((q.shape[1] // BLOCK_Q, KEY_ROWS, BLOCK_Q), jnp.float32),
        ],
        name="attend_blocks",
    )(q, *pieces)


def turned_ring(x, away):
    size = lax.axis_size("sp")
    return lax.ppermute(
        x,
        "sp",
        [(i, i // SEQ_SHARDS * SEQ_SHARDS + (i + away) % SEQ_SHARDS) for i in range(size)],
    )


def layer_norm(values, gain_vec, bias_vec):
    center = jnp.mean(values, axis=-1, keepdims=True)
    shifted = values - center
    variance = jnp.mean(shifted * shifted, axis=-1, keepdims=True)
    return (shifted * lax.rsqrt(variance + EPS_LAYER) * gain_vec + bias_vec).astype(jnp.bfloat16)


def local(
    residual,
    wide_query,
    narrow_query,
    wide_keys,
    narrow_keys,
    wide_values,
    narrow_values,
    wide_query_gain,
    wide_key_gain,
    narrow_query_gain,
    narrow_key_gain,
    wide_out,
    narrow_out,
    first_gain,
    first_bias,
    route_ids,
    route_weights,
    expert_gate,
    expert_up,
    expert_down,
    shared_gate,
    shared_up,
    shared_down,
    second_gain,
    second_bias,
):
    tp_size = lax.axis_size("tp")
    place = jnp.stack(
        [
            lax.axis_index("tp"),
            lax.axis_index("sp") % SEQ_SHARDS * (wide_query.shape[0] // GRID_WIDTH),
        ]
    )
    out_weights = lax.all_gather(
        jnp.concatenate([wide_out, narrow_out], axis=0), "tp", axis=0, tiled=True
    )
    rotated_queries, own_pack = prepare(
        place,
        wide_query.T,
        narrow_query.T,
        wide_keys,
        narrow_keys,
        wide_values,
        narrow_values,
        wide_query_gain,
        wide_key_gain,
        narrow_query_gain,
        narrow_key_gain,
    )
    packs = [own_pack] + [turned_ring(own_pack, away) for away in range(1, SEQ_SHARDS)]
    mixed = attend(rotated_queries, packs)
    tokens = lax.all_to_all(mixed, "tp", split_axis=0, concat_axis=1, tiled=True)
    projected = jnp.dot(tokens, out_weights, preferred_element_type=jnp.float32)
    hidden = layer_norm(ALPHA * residual.astype(jnp.float32) + projected, first_gain, first_bias)
    device_rows = hidden.shape[0]
    model_width = hidden.shape[1]
    sp_size = lax.axis_size("sp")
    top_count = route_ids.shape[1]
    experts = LOCAL_EXPERTS * sp_size
    capacity = max(2, (5 * device_rows * top_count + 4 * experts - 1) // (4 * experts))
    flat_ids = route_ids.reshape(-1)
    expert_hits = (flat_ids[:, None] == jnp.arange(experts, dtype=jnp.int32)[None, :]).astype(
        jnp.int32
    )
    earlier = jnp.sum((jnp.cumsum(expert_hits, axis=0) - expert_hits) * expert_hits, axis=1)
    slot_index = flat_ids * capacity + earlier
    chosen = (
        slot_index[:, None] == jnp.arange(experts * capacity, dtype=jnp.int32)[None, :]
    ).astype(jnp.float32)
    chosen = chosen.reshape(device_rows, top_count, experts * capacity)
    placing = jnp.sum(chosen, axis=1).astype(jnp.bfloat16)
    mixing = jnp.sum(chosen * route_weights[:, :, None], axis=1)
    outgoing = jnp.einsum("rs,rd->sd", placing, hidden, preferred_element_type=jnp.float32).astype(
        jnp.bfloat16
    )
    outgoing = outgoing.reshape(sp_size, LOCAL_EXPERTS, capacity, model_width)
    piece_rows = lax.all_gather(
        lax.all_to_all(outgoing, "sp", split_axis=0, concat_axis=0, tiled=True),
        "tp",
        axis=0,
        tiled=True,
    )
    gate_values = jnp.einsum(
        "secd,edf->secf", piece_rows, expert_gate, preferred_element_type=jnp.float32
    )
    up_values = jnp.einsum(
        "secd,edf->secf", piece_rows, expert_up, preferred_element_type=jnp.float32
    )
    active = (jax.nn.silu(gate_values) * up_values).astype(jnp.bfloat16)
    partial_value = jnp.einsum(
        "secf,efd->secd", active, expert_down, preferred_element_type=jnp.float32
    )
    rounded = lax.optimization_barrier(partial_value.astype(jnp.bfloat16))
    partials = rounded.astype(jnp.float32)
    summed = lax.psum_scatter(partials.astype(jnp.bfloat16), "tp", scatter_dimension=0, tiled=True)
    returned = lax.all_to_all(summed, "sp", split_axis=0, concat_axis=0, tiled=True)
    routed = jnp.dot(mixing, returned.reshape(-1, model_width).astype(jnp.float32))
    shared_gate_values = jnp.dot(hidden, shared_gate, preferred_element_type=jnp.float32)
    shared_up_values = jnp.dot(hidden, shared_up, preferred_element_type=jnp.float32)
    shared_active = (jax.nn.silu(shared_gate_values) * shared_up_values).astype(jnp.bfloat16)
    shared_output = jnp.dot(shared_active, shared_down, preferred_element_type=jnp.float32)
    return layer_norm(
        ALPHA * hidden.astype(jnp.float32) + routed + shared_output, second_gain, second_bias
    )


def solution(mesh):
    in_specs = (
        P(("sp", "tp"), None),
        P("sp", "tp"),
        P("sp", "tp"),
        P("sp", None),
        P("sp", None),
        P("sp", None),
        P("sp", None),
        P(),
        P(),
        P(),
        P(),
        P("tp", None),
        P("tp", None),
        P(),
        P(),
        P(("sp", "tp"), None),
        P(("sp", "tp"), None),
        P("sp", None, "tp"),
        P("sp", None, "tp"),
        P("sp", "tp", None),
        P(),
        P(),
        P(),
        P(),
        P(),
    )
    out_specs = P(("sp", "tp"), None)
    return jax.shard_map(local, mesh=mesh, in_specs=in_specs, out_specs=out_specs, check_vma=False)
```

```python
import jax
import jax.numpy as jnp
from jax import lax
from jax.experimental import pallas as pl
from jax.experimental.pallas import tpu as pltpu
from jax.sharding import PartitionSpec as P

LOCAL_EXPERTS = 2
EPS_LAYER = 1e-05
ALPHA = 2.0**0.25
EPS_HEAD = 1e-06
THETA = 10000.0
GRID_WIDTH = 64
SEQ_SHARDS = 4
LOG2E = 1.4426950408889634
WIDE_SIZE = 64
NARROW_SIZE = 32
KEY_ROWS = WIDE_SIZE + NARROW_SIZE
ONES_ROWS = 16
BLOCK_Q = 256
CHUNK = 512


def column(ref):
    size = ref.shape[1]
    spread = jnp.broadcast_to(ref[...], (size, size))
    diagonal = lax.broadcasted_iota(jnp.int32, (size, size), 0) == lax.broadcasted_iota(
        jnp.int32, (size, size), 1
    )
    return jnp.sum(jnp.where(diagonal, spread, 0.0), axis=1, keepdims=True)


def normed(heads, gain):
    mean_square = jnp.mean(heads * heads, axis=0, keepdims=True)
    return heads * lax.rsqrt(mean_square + EPS_HEAD) * gain


def turned(heads, tables):
    n = heads.shape[0] // 4
    parts = []
    for half, (cosine, sine) in enumerate(tables):
        a = heads[2 * half * n : (2 * half + 1) * n]
        b = heads[(2 * half + 1) * n : (2 * half + 2) * n]
        parts += [a * cosine - b * sine, b * cosine + a * sine]
    return jnp.concatenate(parts, axis=0)


def angle_tables(quarter, first_row, tokens):
    frequency = jnp.exp(
        lax.broadcasted_iota(jnp.int32, (quarter, tokens), 0).astype(jnp.float32)
        * (-jnp.log(jnp.float32(THETA)) / quarter)
    )
    token = lax.broadcasted_iota(jnp.int32, (quarter, tokens), 1)
    row_angle = (token // GRID_WIDTH + first_row).astype(jnp.float32) * frequency
    col_angle = (token % GRID_WIDTH).astype(jnp.float32) * frequency
    return ((jnp.cos(row_angle), jnp.sin(row_angle)), (jnp.cos(col_angle), jnp.sin(col_angle)))


def prepare_kernel(place, wqt, nqt, wk, nk, wv, nv, wqg, wkg, nqg, nkg, q_out, kv_out, turn):
    tokens = wqt.shape[1]
    tp = place[0]
    first_row = place[1]
    wide_tables = angle_tables(WIDE_SIZE // 4, first_row, tokens)
    narrow_tables = angle_tables(NARROW_SIZE // 4, first_row, tokens)

    def picked(ref, start, size):
        block = start // 128
        columns = ref[:, pl.ds(pl.multiple_of(block * 128, 128), 128)]
        turn[...] = columns.astype(jnp.float32).T
        return turn[pl.ds(pl.multiple_of(start % 128, size), size), :]

    wide_start = tp // 4 * WIDE_SIZE
    narrow_start = tp // 2 * NARROW_SIZE
    keys = turned(normed(picked(wk, wide_start, WIDE_SIZE), column(wkg)), wide_tables)
    kv_out[0:64, :] = keys.astype(jnp.bfloat16)
    keys = turned(normed(picked(nk, narrow_start, NARROW_SIZE), column(nkg)), narrow_tables)
    kv_out[64:96, :] = keys.astype(jnp.bfloat16)
    kv_out[96:160, :] = picked(wv, wide_start, WIDE_SIZE).astype(jnp.bfloat16)
    kv_out[160:192, :] = picked(nv, narrow_start, NARROW_SIZE).astype(jnp.bfloat16)
    wide = turned(normed(wqt[...].astype(jnp.float32), column(wqg)), wide_tables)
    q_out[0:64, 0:tokens] = wide.astype(jnp.bfloat16)
    q_out[64:128, 0:tokens] = jnp.zeros((64, tokens), jnp.bfloat16)
    q_out[0:64, tokens:] = jnp.zeros((64, 2 * tokens), jnp.bfloat16)
    q_out[96:128, tokens:] = jnp.zeros((32, 2 * tokens), jnp.bfloat16)
    for head in range(2):
        rows = nqt[NARROW_SIZE * head : NARROW_SIZE * (head + 1), :].astype(jnp.float32)
        narrow = turned(normed(rows, column(nqg)), narrow_tables)
        q_out[64:96, tokens * (head + 1) : tokens * (head + 2)] = narrow.astype(jnp.bfloat16)


def prepare(place, wqt, nqt, wk, nk, wv, nv, wqg, wkg, nqg, nkg):
    tokens = wqt.shape[1]
    vmem = pl.BlockSpec(memory_space=pltpu.VMEM)
    return pl.pallas_call(
        prepare_kernel,
        out_shape=(
            jax.ShapeDtypeStruct((128, 3 * tokens), jnp.bfloat16),
            jax.ShapeDtypeStruct((192, tokens), jnp.bfloat16),
        ),
        in_specs=[pl.BlockSpec(memory_space=pltpu.SMEM)] + [vmem] * 10,
        out_specs=(vmem, vmem),
        scratch_shapes=[pltpu.VMEM((128, tokens), jnp.float32)],
        name="prepare_heads",
    )(
        place, wqt, nqt, wk, nk, wv, nv,
        wqg.reshape(1, -1), wkg.reshape(1, -1), nqg.reshape(1, -1), nkg.reshape(1, -1),
    )


def attend_kernel(q, kv0, kv1, kv2, kv3, out, keys, values, scores0, scores1, mixed):
    tokens = kv0.shape[1]
    total = 4 * tokens
    blocks = q.shape[1] // BLOCK_Q
    wide_blocks = tokens // BLOCK_Q
    values[KEY_ROWS:, :] = jnp.ones((ONES_ROWS, total), jnp.bfloat16)
    for n, kv in enumerate((kv0, kv1, kv2, kv3)):
        piece = kv[0:KEY_ROWS, :].astype(jnp.float32)
        padded = jnp.concatenate([piece, jnp.zeros((128 - KEY_ROWS, tokens), jnp.float32)], axis=0)
        keys[n * tokens : (n + 1) * tokens, :] = padded.T.astype(jnp.bfloat16)
        values[0:KEY_ROWS, n * tokens : (n + 1) * tokens] = kv[KEY_ROWS:, :]

    def scored(c, query, into, largest):
        part = jnp.dot(
            keys[c * CHUNK : (c + 1) * CHUNK, :], query, preferred_element_type=jnp.float32
        )
        into[c * CHUNK : (c + 1) * CHUNK, :] = part
        return jnp.maximum(largest, jnp.max(part.reshape(CHUNK // 8, 8, BLOCK_Q), axis=0))

    lowest = jnp.full((8, BLOCK_Q), -jnp.inf, jnp.float32)
    query_at = lambda b: q[:, pl.ds(pl.multiple_of(b * BLOCK_Q, BLOCK_Q), BLOCK_Q)]

    def step(b, current, following, largest):
        query = query_at(jnp.minimum(b + 1, blocks - 1))
        peak = jnp.max(largest, axis=0, keepdims=True)
        factor = jnp.where(
            b < wide_blocks,
            jnp.float32(WIDE_SIZE**-0.5 * LOG2E),
            jnp.float32(NARROW_SIZE**-0.5 * LOG2E),
        )
        next_largest = lowest
        total_mixed = jnp.zeros((KEY_ROWS + ONES_ROWS, BLOCK_Q), jnp.float32)
        for c in range(total // CHUNK):
            next_largest = scored(c, query, following, next_largest)
            raw = current[c * CHUNK : (c + 1) * CHUNK, :]
            weights = jnp.exp2((raw - peak) * factor).astype(jnp.bfloat16)
            total_mixed = total_mixed + jnp.dot(
                values[:, c * CHUNK : (c + 1) * CHUNK], weights, preferred_element_type=jnp.float32
            )
        mixed[b] = total_mixed[:KEY_ROWS] / total_mixed[KEY_ROWS : KEY_ROWS + 1]
        return next_largest

    largest = lowest
    first = query_at(0)
    for c in range(total // CHUNK):
        largest = scored(c, first, scores0, largest)

    def pair(i, largest):
        largest = step(2 * i, scores0, scores1, largest)
        return step(2 * i + 1, scores1, scores0, largest)

    lax.fori_loop(0, blocks // 2, pair, largest)
    for b in range(wide_blocks):
        rows = jnp.concatenate(
            [
                mixed[b, 0:WIDE_SIZE],
                mixed[wide_blocks + b, WIDE_SIZE:KEY_ROWS],
                mixed[2 * wide_blocks + b, WIDE_SIZE:KEY_ROWS],
            ],
            axis=0,
        )
        out[b * BLOCK_Q : (b + 1) * BLOCK_Q, :] = rows.T.astype(jnp.bfloat16)


def attend(q, pieces):
    tokens = pieces[0].shape[1]
    vmem = pl.BlockSpec(memory_space=pltpu.VMEM)
    return pl.pallas_call(
        attend_kernel,
        out_shape=jax.ShapeDtypeStruct((tokens, 128), jnp.bfloat16),
        in_specs=[vmem] * 5,
        out_specs=vmem,
        scratch_shapes=[
            pltpu.VMEM((4 * tokens, 128), jnp.bfloat16),
            pltpu.VMEM((KEY_ROWS + ONES_ROWS, 4 * tokens), jnp.bfloat16),
            pltpu.VMEM((4 * tokens, BLOCK_Q), jnp.float32),
            pltpu.VMEM((4 * tokens, BLOCK_Q), jnp.float32),
            pltpu.VMEM((q.shape[1] // BLOCK_Q, KEY_ROWS, BLOCK_Q), jnp.float32),
        ],
        name="attend_blocks",
    )(q, *pieces)


def expert_kernel(rows, gate, up, down, out):
    e = pl.program_id(0)
    sources, _, slots, width = rows.shape
    x = rows[...].reshape(sources * slots, width)
    along = (((1,), (1,)), ((), ()))
    gate_values = lax.dot_general(x, gate[e], along, preferred_element_type=jnp.float32)
    up_values = lax.dot_general(x, up[e], along, preferred_element_type=jnp.float32)
    active = gate_values / (1.0 + jnp.exp(-gate_values)) * up_values
    partial_value = jnp.dot(
        active.astype(jnp.bfloat16), down[e], preferred_element_type=jnp.float32
    )
    out[...] = partial_value.astype(jnp.bfloat16).reshape(rows.shape)


def run_experts(rows, gate, up, down):
    sources, experts, slots, width = rows.shape
    block = pl.BlockSpec((sources // 4, 1, slots, width), lambda e, r: (r, e, 0, 0))
    whole = pl.BlockSpec(memory_space=pltpu.VMEM)
    return pl.pallas_call(
        expert_kernel,
        grid=(experts, 4),
        out_shape=jax.ShapeDtypeStruct(rows.shape, jnp.bfloat16),
        in_specs=[block, whole, whole, whole],
        out_specs=block,
        name="run_experts",
    )(rows, gate, up, down)


def turned_ring(x, away):
    size = lax.axis_size("sp")
    return lax.ppermute(
        x,
        "sp",
        [(i, i // SEQ_SHARDS * SEQ_SHARDS + (i + away) % SEQ_SHARDS) for i in range(size)],
    )


def layer_norm(values, gain_vec, bias_vec):
    center = jnp.mean(values, axis=-1, keepdims=True)
    shifted = values - center
    variance = jnp.mean(shifted * shifted, axis=-1, keepdims=True)
    return (shifted * lax.rsqrt(variance + EPS_LAYER) * gain_vec + bias_vec).astype(jnp.bfloat16)


def local(
    residual,
    wide_query,
    narrow_query,
    wide_keys,
    narrow_keys,
    wide_values,
    narrow_values,
    wide_query_gain,
    wide_key_gain,
    narrow_query_gain,
    narrow_key_gain,
    wide_out,
    narrow_out,
    first_gain,
    first_bias,
    route_ids,
    route_weights,
    expert_gate,
    expert_up,
    expert_down,
    shared_gate,
    shared_up,
    shared_down,
    second_gain,
    second_bias,
):
    tp_size = lax.axis_size("tp")
    place = jnp.stack(
        [
            lax.axis_index("tp"),
            lax.axis_index("sp") % SEQ_SHARDS * (wide_query.shape[0] // GRID_WIDTH),
        ]
    )
    out_weights = lax.all_gather(
        jnp.concatenate([wide_out, narrow_out], axis=0), "tp", axis=0, tiled=True
    )
    rotated_queries, own_pack = prepare(
        place,
        wide_query.T,
        narrow_query.T,
        wide_keys,
        narrow_keys,
        wide_values,
        narrow_values,
        wide_query_gain,
        wide_key_gain,
        narrow_query_gain,
        narrow_key_gain,
    )
    packs = [own_pack] + [turned_ring(own_pack, away) for away in range(1, SEQ_SHARDS)]
    mixed = attend(rotated_queries, packs)
    tokens = lax.all_to_all(mixed, "tp", split_axis=0, concat_axis=1, tiled=True)
    projected = jnp.dot(tokens, out_weights, preferred_element_type=jnp.float32)
    hidden = layer_norm(ALPHA * residual.astype(jnp.float32) + projected, first_gain, first_bias)
    device_rows = hidden.shape[0]
    model_width = hidden.shape[1]
    sp_size = lax.axis_size("sp")
    top_count = route_ids.shape[1]
    experts = LOCAL_EXPERTS * sp_size
    capacity = max(2, (5 * device_rows * top_count + 4 * experts - 1) // (4 * experts))
    flat_ids = route_ids.reshape(-1)
    expert_hits = (flat_ids[:, None] == jnp.arange(experts, dtype=jnp.int32)[None, :]).astype(
        jnp.int32
    )
    earlier = jnp.sum((jnp.cumsum(expert_hits, axis=0) - expert_hits) * expert_hits, axis=1)
    slot_index = flat_ids * capacity + earlier
    chosen = (
        slot_index[:, None] == jnp.arange(experts * capacity, dtype=jnp.int32)[None, :]
    ).astype(jnp.float32)
    chosen = chosen.reshape(device_rows, top_count, experts * capacity)
    placing = jnp.sum(chosen, axis=1).astype(jnp.bfloat16)
    mixing = jnp.sum(chosen * route_weights[:, :, None], axis=1)
    outgoing = jnp.einsum("rs,rd->sd", placing, hidden, preferred_element_type=jnp.float32).astype(
        jnp.bfloat16
    )
    outgoing = outgoing.reshape(sp_size, LOCAL_EXPERTS, capacity, model_width)
    arrived = lax.all_to_all(outgoing, "sp", split_axis=0, concat_axis=0, tiled=True)
    slab = jnp.transpose(arrived, (1, 2, 0, 3)).reshape(
        LOCAL_EXPERTS, capacity * sp_size, model_width
    )
    piece_rows = lax.all_gather(slab, "tp", axis=0, tiled=False)
    partial_value = run_experts(
        piece_rows,
        jnp.transpose(expert_gate, (0, 2, 1)),
        jnp.transpose(expert_up, (0, 2, 1)),
        expert_down,
    )
    summed = lax.psum_scatter(partial_value, "tp", scatter_dimension=0, tiled=False)
    summed = summed.reshape(LOCAL_EXPERTS, capacity, sp_size, model_width)
    returned = lax.all_to_all(
        jnp.transpose(summed, (2, 0, 1, 3)), "sp", split_axis=0, concat_axis=0, tiled=True
    )
    routed = jnp.dot(mixing, returned.reshape(-1, model_width).astype(jnp.float32))
    shared_gate_values = jnp.dot(hidden, shared_gate, preferred_element_type=jnp.float32)
    shared_up_values = jnp.dot(hidden, shared_up, preferred_element_type=jnp.float32)
    shared_active = (jax.nn.silu(shared_gate_values) * shared_up_values).astype(jnp.bfloat16)
    shared_output = jnp.dot(shared_active, shared_down, preferred_element_type=jnp.float32)
    return layer_norm(
        ALPHA * hidden.astype(jnp.float32) + routed + shared_output, second_gain, second_bias
    )


def solution(mesh):
    in_specs = (
        P(("sp", "tp"), None),
        P("sp", "tp"),
        P("sp", "tp"),
        P("sp", None),
        P("sp", None),
        P("sp", None),
        P("sp", None),
        P(),
        P(),
        P(),
        P(),
        P("tp", None),
        P("tp", None),
        P(),
        P(),
        P(("sp", "tp"), None),
        P(("sp", "tp"), None),
        P("sp", None, "tp"),
        P("sp", None, "tp"),
        P("sp", "tp", None),
        P(),
        P(),
        P(),
        P(),
        P(),
    )
    out_specs = P(("sp", "tp"), None)
    return jax.shard_map(local, mesh=mesh, in_specs=in_specs, out_specs=out_specs, check_vma=False)
```

```python
import functools

import jax
import jax.numpy as jnp
from jax import lax
from jax.experimental import pallas as pl
from jax.experimental.pallas import tpu as pltpu
from jax.sharding import PartitionSpec as P

LOCAL_EXPERTS = 2
EPS_LAYER = 1e-05
ALPHA = 2.0**0.25
EPS_HEAD = 1e-06
THETA = 10000.0
GRID_WIDTH = 64
SEQ_SHARDS = 4
LOG2E = 1.4426950408889634
WIDE_SIZE = 64
NARROW_SIZE = 32
KEY_ROWS = WIDE_SIZE + NARROW_SIZE
ONES_ROWS = 16
BLOCK_Q = 256
CHUNK = 512


def column(ref):
    size = ref.shape[1]
    spread = jnp.broadcast_to(ref[...], (size, size))
    diagonal = lax.broadcasted_iota(jnp.int32, (size, size), 0) == lax.broadcasted_iota(
        jnp.int32, (size, size), 1
    )
    return jnp.sum(jnp.where(diagonal, spread, 0.0), axis=1, keepdims=True)


def normed(heads, gain):
    mean_square = jnp.mean(heads * heads, axis=0, keepdims=True)
    return heads * lax.rsqrt(mean_square + EPS_HEAD) * gain


def turned(heads, tables):
    n = heads.shape[0] // 4
    parts = []
    for half, (cosine, sine) in enumerate(tables):
        a = heads[2 * half * n : (2 * half + 1) * n]
        b = heads[(2 * half + 1) * n : (2 * half + 2) * n]
        parts += [a * cosine - b * sine, b * cosine + a * sine]
    return jnp.concatenate(parts, axis=0)


def angle_tables(quarter, first_row, tokens):
    frequency = jnp.exp(
        lax.broadcasted_iota(jnp.int32, (quarter, tokens), 0).astype(jnp.float32)
        * (-jnp.log(jnp.float32(THETA)) / quarter)
    )
    token = lax.broadcasted_iota(jnp.int32, (quarter, tokens), 1)
    row_angle = (token // GRID_WIDTH + first_row).astype(jnp.float32) * frequency
    col_angle = (token % GRID_WIDTH).astype(jnp.float32) * frequency
    return ((jnp.cos(row_angle), jnp.sin(row_angle)), (jnp.cos(col_angle), jnp.sin(col_angle)))


def prepare_kernel(wqt, nqt, wk, nk, wv, nv, wqg, wkg, nqg, nkg, q_out, kv_out, turn):
    tokens = wqt.shape[1]
    tp = lax.axis_index("tp")
    first_row = lax.axis_index("sp") % SEQ_SHARDS * (tokens // GRID_WIDTH)
    wide_tables = angle_tables(WIDE_SIZE // 4, first_row, tokens)
    narrow_tables = angle_tables(NARROW_SIZE // 4, first_row, tokens)

    def picked(ref, start, size):
        block = start // 128
        columns = ref[:, pl.ds(pl.multiple_of(block * 128, 128), 128)]
        turn[...] = columns.astype(jnp.float32).T
        return turn[pl.ds(pl.multiple_of(start % 128, size), size), :]

    wide_start = tp // 4 * WIDE_SIZE
    narrow_start = tp // 2 * NARROW_SIZE
    keys = turned(normed(picked(wk, wide_start, WIDE_SIZE), column(wkg)), wide_tables)
    kv_out[0:64, :] = keys.astype(jnp.bfloat16)
    keys = turned(normed(picked(nk, narrow_start, NARROW_SIZE), column(nkg)), narrow_tables)
    kv_out[64:96, :] = keys.astype(jnp.bfloat16)
    kv_out[96:160, :] = picked(wv, wide_start, WIDE_SIZE).astype(jnp.bfloat16)
    kv_out[160:192, :] = picked(nv, narrow_start, NARROW_SIZE).astype(jnp.bfloat16)
    wide = turned(normed(wqt[...].astype(jnp.float32), column(wqg)), wide_tables)
    q_out[0:64, 0:tokens] = wide.astype(jnp.bfloat16)
    q_out[64:128, 0:tokens] = jnp.zeros((64, tokens), jnp.bfloat16)
    q_out[0:64, tokens:] = jnp.zeros((64, 2 * tokens), jnp.bfloat16)
    q_out[96:128, tokens:] = jnp.zeros((32, 2 * tokens), jnp.bfloat16)
    for head in range(2):
        rows = nqt[NARROW_SIZE * head : NARROW_SIZE * (head + 1), :].astype(jnp.float32)
        narrow = turned(normed(rows, column(nqg)), narrow_tables)
        q_out[64:96, tokens * (head + 1) : tokens * (head + 2)] = narrow.astype(jnp.bfloat16)


def prepare(wqt, nqt, wk, nk, wv, nv, wqg, wkg, nqg, nkg):
    tokens = wqt.shape[1]
    vmem = pl.BlockSpec(memory_space=pltpu.VMEM)
    return pl.pallas_call(
        prepare_kernel,
        out_shape=(
            jax.ShapeDtypeStruct((128, 3 * tokens), jnp.bfloat16),
            jax.ShapeDtypeStruct((192, tokens), jnp.bfloat16),
        ),
        in_specs=[vmem] * 10,
        out_specs=(vmem, vmem),
        scratch_shapes=[pltpu.VMEM((128, tokens), jnp.float32)],
        name="prepare_heads",
    )(
        wqt, nqt, wk, nk, wv, nv,
        wqg.reshape(1, -1), wkg.reshape(1, -1), nqg.reshape(1, -1), nkg.reshape(1, -1),
    )


def attend_kernel(*refs, pieces, resumed):
    q = refs[0]
    packs = refs[1 : 1 + pieces]
    refs = refs[1 + pieces :]
    if resumed:
        before, peak_before, out, keys, values, scores0, scores1, mixed = refs
    else:
        sums, peaks, keys, values, scores0, scores1 = refs
    tokens = packs[0].shape[1]
    total = pieces * tokens
    blocks = q.shape[1] // BLOCK_Q
    wide_blocks = tokens // BLOCK_Q
    values[KEY_ROWS:, :] = jnp.ones((ONES_ROWS, total), jnp.bfloat16)
    for n, kv in enumerate(packs):
        piece = kv[0:KEY_ROWS, :].astype(jnp.float32)
        padded = jnp.concatenate([piece, jnp.zeros((128 - KEY_ROWS, tokens), jnp.float32)], axis=0)
        keys[n * tokens : (n + 1) * tokens, :] = padded.T.astype(jnp.bfloat16)
        values[0:KEY_ROWS, n * tokens : (n + 1) * tokens] = kv[KEY_ROWS:, :]

    def scored(c, query, into, largest):
        part = jnp.dot(
            keys[c * CHUNK : (c + 1) * CHUNK, :], query, preferred_element_type=jnp.float32
        )
        into[c * CHUNK : (c + 1) * CHUNK, :] = part
        return jnp.maximum(largest, jnp.max(part.reshape(CHUNK // 8, 8, BLOCK_Q), axis=0))

    lowest = jnp.full((8, BLOCK_Q), -jnp.inf, jnp.float32)
    query_at = lambda b: q[:, pl.ds(pl.multiple_of(b * BLOCK_Q, BLOCK_Q), BLOCK_Q)]

    def step(b, current, following, largest):
        query = query_at(jnp.minimum(b + 1, blocks - 1))
        peak = jnp.max(largest, axis=0, keepdims=True)
        factor = jnp.where(
            b < wide_blocks,
            jnp.float32(WIDE_SIZE**-0.5 * LOG2E),
            jnp.float32(NARROW_SIZE**-0.5 * LOG2E),
        )
        if resumed:
            earlier = peak_before[b][0:1]
            peak = jnp.maximum(peak, earlier)
            total_mixed = before[b] * jnp.exp2((earlier - peak) * factor)
        else:
            total_mixed = jnp.zeros((KEY_ROWS + ONES_ROWS, BLOCK_Q), jnp.float32)
        next_largest = lowest
        for c in range(total // CHUNK):
            next_largest = scored(c, query, following, next_largest)
            raw = current[c * CHUNK : (c + 1) * CHUNK, :]
            weights = jnp.exp2((raw - peak) * factor).astype(jnp.bfloat16)
            total_mixed = total_mixed + jnp.dot(
                values[:, c * CHUNK : (c + 1) * CHUNK], weights, preferred_element_type=jnp.float32
            )
        if resumed:
            mixed[b] = total_mixed[:KEY_ROWS] / total_mixed[KEY_ROWS : KEY_ROWS + 1]
        else:
            sums[b] = total_mixed
            peaks[b] = jnp.broadcast_to(peak, (8, BLOCK_Q))
        return next_largest

    largest = lowest
    first = query_at(0)
    for c in range(total // CHUNK):
        largest = scored(c, first, scores0, largest)

    def pair(i, largest):
        largest = step(2 * i, scores0, scores1, largest)
        return step(2 * i + 1, scores1, scores0, largest)

    lax.fori_loop(0, blocks // 2, pair, largest)
    if not resumed:
        return
    for b in range(wide_blocks):
        rows = jnp.concatenate(
            [
                mixed[b, 0:WIDE_SIZE],
                mixed[wide_blocks + b, WIDE_SIZE:KEY_ROWS],
                mixed[2 * wide_blocks + b, WIDE_SIZE:KEY_ROWS],
            ],
            axis=0,
        )
        out[b * BLOCK_Q : (b + 1) * BLOCK_Q, :] = rows.T.astype(jnp.bfloat16)


def attend(q, packs, earlier=()):
    tokens = packs[0].shape[1]
    total = len(packs) * tokens
    blocks = q.shape[1] // BLOCK_Q
    sums = jax.ShapeDtypeStruct((blocks, KEY_ROWS + ONES_ROWS, BLOCK_Q), jnp.float32)
    peaks = jax.ShapeDtypeStruct((blocks, 8, BLOCK_Q), jnp.float32)
    vmem = pl.BlockSpec(memory_space=pltpu.VMEM)
    scratch = [
        pltpu.VMEM((total, 128), jnp.bfloat16),
        pltpu.VMEM((KEY_ROWS + ONES_ROWS, total), jnp.bfloat16),
        pltpu.VMEM((total, BLOCK_Q), jnp.float32),
        pltpu.VMEM((total, BLOCK_Q), jnp.float32),
    ]
    if earlier:
        scratch.append(pltpu.VMEM((blocks, KEY_ROWS, BLOCK_Q), jnp.float32))
    return pl.pallas_call(
        functools.partial(attend_kernel, pieces=len(packs), resumed=bool(earlier)),
        out_shape=jax.ShapeDtypeStruct((tokens, 128), jnp.bfloat16) if earlier else (sums, peaks),
        in_specs=[vmem] * (1 + len(packs) + len(earlier)),
        out_specs=vmem if earlier else (vmem, vmem),
        scratch_shapes=scratch,
        name="attend_rest" if earlier else "attend_first",
    )(q, *packs, *earlier)


def stack_kernel(first, second, out):
    out[: first.shape[0]] = first[...]
    out[first.shape[0] :] = second[...]


def stacked(first, second):
    vmem = pl.BlockSpec(memory_space=pltpu.VMEM)
    return pl.pallas_call(
        stack_kernel,
        out_shape=jax.ShapeDtypeStruct((2 * first.shape[0], first.shape[1]), first.dtype),
        in_specs=[vmem, vmem],
        out_specs=vmem,
        name="stack_rows",
    )(first, second)


def expert_kernel(rows, gate, gate_far, up, up_far, down, down_far, out):
    sources, _, slots, width = rows.shape
    x = rows[...].reshape(sources * slots, width)
    along = (((1,), (1,)), ((), ()))
    partial_value = jnp.zeros(x.shape, jnp.float32)
    for g, u, d in ((gate, up, down), (gate_far, up_far, down_far)):
        gate_values = lax.dot_general(x, g[0], along, preferred_element_type=jnp.float32)
        up_values = lax.dot_general(x, u[0], along, preferred_element_type=jnp.float32)
        active = gate_values / (1.0 + jnp.exp(-gate_values)) * up_values
        partial_value = partial_value + jnp.dot(
            active.astype(jnp.bfloat16), d[0], preferred_element_type=jnp.float32
        )
    out[...] = partial_value.astype(jnp.bfloat16).reshape(rows.shape)


def run_experts(rows, *weights):
    sources, experts, slots, width = rows.shape
    block = pl.BlockSpec((sources // 2, 1, slots, width), lambda e, r: (r, e, 0, 0))
    weight = pl.BlockSpec((1, *weights[0].shape[1:]), lambda e, r: (e, 0, 0))
    return pl.pallas_call(
        expert_kernel,
        grid=(experts, 2),
        out_shape=jax.ShapeDtypeStruct(rows.shape, jnp.bfloat16),
        in_specs=[block] + [weight] * len(weights),
        out_specs=block,
        name="run_experts",
    )(rows, *weights)


def other_core(x):
    return lax.ppermute(x, "tp", [(i, i ^ 1) for i in range(lax.axis_size("tp"))])


def turned_ring(x, away):
    size = lax.axis_size("sp")
    return lax.ppermute(
        x,
        "sp",
        [(i, i // SEQ_SHARDS * SEQ_SHARDS + (i + away) % SEQ_SHARDS) for i in range(size)],
    )


def layer_norm(values, gain_vec, bias_vec):
    center = jnp.mean(values, axis=-1, keepdims=True)
    shifted = values - center
    variance = jnp.mean(shifted * shifted, axis=-1, keepdims=True)
    return (shifted * lax.rsqrt(variance + EPS_LAYER) * gain_vec + bias_vec).astype(jnp.bfloat16)


def local(
    residual,
    wide_query,
    narrow_query,
    wide_keys,
    narrow_keys,
    wide_values,
    narrow_values,
    wide_query_gain,
    wide_key_gain,
    narrow_query_gain,
    narrow_key_gain,
    wide_out,
    narrow_out,
    first_gain,
    first_bias,
    route_ids,
    route_weights,
    expert_gate,
    expert_up,
    expert_down,
    shared_gate,
    shared_up,
    shared_down,
    second_gain,
    second_bias,
):
    tp_size = lax.axis_size("tp")
    out_weights = lax.all_gather(
        stacked(wide_out, narrow_out), "tp", axis=0, tiled=True
    )
    rotated_queries, own_pack = prepare(
        wide_query.T,
        narrow_query.T,
        wide_keys,
        narrow_keys,
        wide_values,
        narrow_values,
        wide_query_gain,
        wide_key_gain,
        narrow_query_gain,
        narrow_key_gain,
    )
    packs = [own_pack] + [turned_ring(own_pack, away) for away in range(1, SEQ_SHARDS)]
    earlier = attend(rotated_queries, packs[:2])
    mixed = attend(rotated_queries, packs[2:], earlier)
    tokens = lax.all_to_all(mixed, "tp", split_axis=0, concat_axis=1, tiled=True)
    projected = jnp.dot(tokens, out_weights, preferred_element_type=jnp.float32)
    hidden = layer_norm(ALPHA * residual.astype(jnp.float32) + projected, first_gain, first_bias)
    device_rows = hidden.shape[0]
    model_width = hidden.shape[1]
    sp_size = lax.axis_size("sp")
    top_count = route_ids.shape[1]
    experts = LOCAL_EXPERTS * sp_size
    capacity = max(2, (5 * device_rows * top_count + 4 * experts - 1) // (4 * experts))
    flat_ids = route_ids.reshape(-1)
    expert_hits = (flat_ids[:, None] == jnp.arange(experts, dtype=jnp.int32)[None, :]).astype(
        jnp.int32
    )
    earlier = jnp.sum((jnp.cumsum(expert_hits, axis=0) - expert_hits) * expert_hits, axis=1)
    slot_index = flat_ids * capacity + earlier
    chosen = (
        slot_index[:, None] == jnp.arange(experts * capacity, dtype=jnp.int32)[None, :]
    ).astype(jnp.float32)
    chosen = chosen.reshape(device_rows, top_count, experts * capacity)
    placing = jnp.sum(chosen, axis=1).astype(jnp.bfloat16)
    mixing = jnp.sum(chosen * route_weights[:, :, None], axis=1)
    outgoing = jnp.einsum("rs,rd->sd", placing, hidden, preferred_element_type=jnp.float32).astype(
        jnp.bfloat16
    )
    outgoing = outgoing.reshape(sp_size, LOCAL_EXPERTS, capacity, model_width)
    arrived = lax.all_to_all(outgoing, "sp", split_axis=0, concat_axis=0, tiled=True)
    slab = jnp.transpose(arrived, (1, 2, 0, 3)).reshape(
        LOCAL_EXPERTS, capacity * sp_size, model_width
    )
    core_lines = [list(range(core, tp_size, 2)) for core in range(2)]
    piece_rows = lax.all_gather(slab, "tp", axis=0, tiled=False, axis_index_groups=core_lines)
    gate_rows = jnp.transpose(expert_gate, (0, 2, 1))
    up_rows = jnp.transpose(expert_up, (0, 2, 1))
    partial_value = run_experts(
        piece_rows,
        gate_rows,
        other_core(gate_rows),
        up_rows,
        other_core(up_rows),
        expert_down,
        other_core(expert_down),
    )
    summed = lax.psum_scatter(
        partial_value, "tp", scatter_dimension=0, tiled=False, axis_index_groups=core_lines
    )
    summed = summed.reshape(LOCAL_EXPERTS, capacity, sp_size, model_width)
    returned = lax.all_to_all(
        jnp.transpose(summed, (2, 0, 1, 3)), "sp", split_axis=0, concat_axis=0, tiled=True
    )
    routed = jnp.dot(mixing, returned.reshape(-1, model_width).astype(jnp.float32))
    shared_gate_values = jnp.dot(hidden, shared_gate, preferred_element_type=jnp.float32)
    shared_up_values = jnp.dot(hidden, shared_up, preferred_element_type=jnp.float32)
    shared_active = (jax.nn.silu(shared_gate_values) * shared_up_values).astype(jnp.bfloat16)
    shared_output = jnp.dot(shared_active, shared_down, preferred_element_type=jnp.float32)
    return layer_norm(
        ALPHA * hidden.astype(jnp.float32) + routed + shared_output, second_gain, second_bias
    )


def solution(mesh):
    in_specs = (
        P(("sp", "tp"), None),
        P("sp", "tp"),
        P("sp", "tp"),
        P("sp", None),
        P("sp", None),
        P("sp", None),
        P("sp", None),
        P(),
        P(),
        P(),
        P(),
        P("tp", None),
        P("tp", None),
        P(),
        P(),
        P(("sp", "tp"), None),
        P(("sp", "tp"), None),
        P("sp", None, "tp"),
        P("sp", None, "tp"),
        P("sp", "tp", None),
        P(),
        P(),
        P(),
        P(),
        P(),
    )
    out_specs = P(("sp", "tp"), None)
    return jax.shard_map(local, mesh=mesh, in_specs=in_specs, out_specs=out_specs, check_vma=False)
```

```python
import functools

import jax
import jax.numpy as jnp
from jax import lax
from jax.experimental import pallas as pl
from jax.experimental.pallas import tpu as pltpu
from jax.sharding import PartitionSpec as P

LOCAL_EXPERTS = 2
EPS_LAYER = 1e-05
ALPHA = 2.0**0.25
EPS_HEAD = 1e-06
THETA = 10000.0
GRID_WIDTH = 64
SEQ_SHARDS = 4
LOG2E = 1.4426950408889634
WIDE_SIZE = 64
NARROW_SIZE = 32
KEY_ROWS = WIDE_SIZE + NARROW_SIZE
ONES_ROWS = 16
BLOCK_Q = 256
CHUNK = 512


def column(ref):
    size = ref.shape[1]
    spread = jnp.broadcast_to(ref[...], (size, size))
    diagonal = lax.broadcasted_iota(jnp.int32, (size, size), 0) == lax.broadcasted_iota(
        jnp.int32, (size, size), 1
    )
    return jnp.sum(jnp.where(diagonal, spread, 0.0), axis=1, keepdims=True)


def normed(heads, gain):
    mean_square = jnp.mean(heads * heads, axis=0, keepdims=True)
    return heads * lax.rsqrt(mean_square + EPS_HEAD) * gain


def turned(heads, tables):
    n = heads.shape[0] // 4
    parts = []
    for half, (cosine, sine) in enumerate(tables):
        a = heads[2 * half * n : (2 * half + 1) * n]
        b = heads[(2 * half + 1) * n : (2 * half + 2) * n]
        parts += [a * cosine - b * sine, b * cosine + a * sine]
    return jnp.concatenate(parts, axis=0)


def angle_tables(quarter, first_row, tokens):
    frequency = jnp.exp(
        lax.broadcasted_iota(jnp.int32, (quarter, tokens), 0).astype(jnp.float32)
        * (-jnp.log(jnp.float32(THETA)) / quarter)
    )
    token = lax.broadcasted_iota(jnp.int32, (quarter, tokens), 1)
    row_angle = (token // GRID_WIDTH + first_row).astype(jnp.float32) * frequency
    col_angle = (token % GRID_WIDTH).astype(jnp.float32) * frequency
    return ((jnp.cos(row_angle), jnp.sin(row_angle)), (jnp.cos(col_angle), jnp.sin(col_angle)))


def prepare_kernel(wqt, nqt, wk, nk, wv, nv, wqg, wkg, nqg, nkg, q_out, kv_out, turn):
    tokens = wqt.shape[1]
    tp = lax.axis_index("tp")
    first_row = lax.axis_index("sp") % SEQ_SHARDS * (tokens // GRID_WIDTH)
    wide_tables = angle_tables(WIDE_SIZE // 4, first_row, tokens)
    narrow_tables = angle_tables(NARROW_SIZE // 4, first_row, tokens)

    def picked(ref, start, size):
        block = start // 128
        columns = ref[:, pl.ds(pl.multiple_of(block * 128, 128), 128)]
        turn[...] = columns.astype(jnp.float32).T
        return turn[pl.ds(pl.multiple_of(start % 128, size), size), :]

    wide_start = tp // 4 * WIDE_SIZE
    narrow_start = tp // 2 * NARROW_SIZE
    keys = turned(normed(picked(wk, wide_start, WIDE_SIZE), column(wkg)), wide_tables)
    kv_out[0:64, :] = keys.astype(jnp.bfloat16)
    keys = turned(normed(picked(nk, narrow_start, NARROW_SIZE), column(nkg)), narrow_tables)
    kv_out[64:96, :] = keys.astype(jnp.bfloat16)
    kv_out[96:160, :] = picked(wv, wide_start, WIDE_SIZE).astype(jnp.bfloat16)
    kv_out[160:192, :] = picked(nv, narrow_start, NARROW_SIZE).astype(jnp.bfloat16)
    wide = turned(normed(wqt[...].astype(jnp.float32), column(wqg)), wide_tables)
    q_out[0:64, 0:tokens] = wide.astype(jnp.bfloat16)
    q_out[64:128, 0:tokens] = jnp.zeros((64, tokens), jnp.bfloat16)
    q_out[0:64, tokens:] = jnp.zeros((64, 2 * tokens), jnp.bfloat16)
    q_out[96:128, tokens:] = jnp.zeros((32, 2 * tokens), jnp.bfloat16)
    for head in range(2):
        rows = nqt[NARROW_SIZE * head : NARROW_SIZE * (head + 1), :].astype(jnp.float32)
        narrow = turned(normed(rows, column(nqg)), narrow_tables)
        q_out[64:96, tokens * (head + 1) : tokens * (head + 2)] = narrow.astype(jnp.bfloat16)


def prepare(wqt, nqt, wk, nk, wv, nv, wqg, wkg, nqg, nkg):
    tokens = wqt.shape[1]
    vmem = pl.BlockSpec(memory_space=pltpu.VMEM)
    return pl.pallas_call(
        prepare_kernel,
        out_shape=(
            jax.ShapeDtypeStruct((128, 3 * tokens), jnp.bfloat16),
            jax.ShapeDtypeStruct((192, tokens), jnp.bfloat16),
        ),
        in_specs=[vmem] * 10,
        out_specs=(vmem, vmem),
        scratch_shapes=[pltpu.VMEM((128, tokens), jnp.float32)],
        name="prepare_heads",
    )(
        wqt, nqt, wk, nk, wv, nv,
        wqg.reshape(1, -1), wkg.reshape(1, -1), nqg.reshape(1, -1), nkg.reshape(1, -1),
    )


def attend_kernel(*refs, pieces, resumed):
    q = refs[0]
    packs = refs[1 : 1 + pieces]
    refs = refs[1 + pieces :]
    if resumed:
        before, peak_before, out, keys, values, scores0, scores1, mixed = refs
    else:
        sums, peaks, keys, values, scores0, scores1 = refs
    tokens = packs[0].shape[1]
    total = pieces * tokens
    blocks = q.shape[1] // BLOCK_Q
    wide_blocks = tokens // BLOCK_Q
    values[KEY_ROWS:, :] = jnp.ones((ONES_ROWS, total), jnp.bfloat16)
    for n, kv in enumerate(packs):
        piece = kv[0:KEY_ROWS, :].astype(jnp.float32)
        padded = jnp.concatenate([piece, jnp.zeros((128 - KEY_ROWS, tokens), jnp.float32)], axis=0)
        keys[n * tokens : (n + 1) * tokens, :] = padded.T.astype(jnp.bfloat16)
        values[0:KEY_ROWS, n * tokens : (n + 1) * tokens] = kv[KEY_ROWS:, :]

    def scored(c, query, into, largest):
        part = jnp.dot(
            keys[c * CHUNK : (c + 1) * CHUNK, :], query, preferred_element_type=jnp.float32
        )
        into[c * CHUNK : (c + 1) * CHUNK, :] = part
        return jnp.maximum(largest, jnp.max(part.reshape(CHUNK // 8, 8, BLOCK_Q), axis=0))

    lowest = jnp.full((8, BLOCK_Q), -jnp.inf, jnp.float32)
    query_at = lambda b: q[:, pl.ds(pl.multiple_of(b * BLOCK_Q, BLOCK_Q), BLOCK_Q)]

    def step(b, current, following, largest):
        query = query_at(jnp.minimum(b + 1, blocks - 1))
        peak = jnp.max(largest, axis=0, keepdims=True)
        factor = jnp.where(
            b < wide_blocks,
            jnp.float32(WIDE_SIZE**-0.5 * LOG2E),
            jnp.float32(NARROW_SIZE**-0.5 * LOG2E),
        )
        if resumed:
            earlier = peak_before[b][0:1]
            peak = jnp.maximum(peak, earlier)
            total_mixed = before[b] * jnp.exp2((earlier - peak) * factor)
        else:
            total_mixed = jnp.zeros((KEY_ROWS + ONES_ROWS, BLOCK_Q), jnp.float32)
        next_largest = lowest
        for c in range(total // CHUNK):
            next_largest = scored(c, query, following, next_largest)
            raw = current[c * CHUNK : (c + 1) * CHUNK, :]
            weights = jnp.exp2((raw - peak) * factor).astype(jnp.bfloat16)
            total_mixed = total_mixed + jnp.dot(
                values[:, c * CHUNK : (c + 1) * CHUNK], weights, preferred_element_type=jnp.float32
            )
        if resumed:
            mixed[b] = total_mixed[:KEY_ROWS] / total_mixed[KEY_ROWS : KEY_ROWS + 1]
        else:
            sums[b] = total_mixed
            peaks[b] = jnp.broadcast_to(peak, (8, BLOCK_Q))
        return next_largest

    largest = lowest
    first = query_at(0)
    for c in range(total // CHUNK):
        largest = scored(c, first, scores0, largest)

    def pair(i, largest):
        largest = step(2 * i, scores0, scores1, largest)
        return step(2 * i + 1, scores1, scores0, largest)

    lax.fori_loop(0, blocks // 2, pair, largest)
    if not resumed:
        return
    for b in range(wide_blocks):
        rows = jnp.concatenate(
            [
                mixed[b, 0:WIDE_SIZE],
                mixed[wide_blocks + b, WIDE_SIZE:KEY_ROWS],
                mixed[2 * wide_blocks + b, WIDE_SIZE:KEY_ROWS],
            ],
            axis=0,
        )
        rows = rows.astype(jnp.bfloat16)
        for n in range(BLOCK_Q // 128):
            out[b * (BLOCK_Q // 128) + n] = rows[:, n * 128 : (n + 1) * 128]


def attend(q, packs, earlier=()):
    tokens = packs[0].shape[1]
    total = len(packs) * tokens
    blocks = q.shape[1] // BLOCK_Q
    sums = jax.ShapeDtypeStruct((blocks, KEY_ROWS + ONES_ROWS, BLOCK_Q), jnp.float32)
    peaks = jax.ShapeDtypeStruct((blocks, 8, BLOCK_Q), jnp.float32)
    vmem = pl.BlockSpec(memory_space=pltpu.VMEM)
    scratch = [
        pltpu.VMEM((total, 128), jnp.bfloat16),
        pltpu.VMEM((KEY_ROWS + ONES_ROWS, total), jnp.bfloat16),
        pltpu.VMEM((total, BLOCK_Q), jnp.float32),
        pltpu.VMEM((total, BLOCK_Q), jnp.float32),
    ]
    if earlier:
        scratch.append(pltpu.VMEM((blocks, KEY_ROWS, BLOCK_Q), jnp.float32))
    return pl.pallas_call(
        functools.partial(attend_kernel, pieces=len(packs), resumed=bool(earlier)),
        out_shape=jax.ShapeDtypeStruct((tokens // 128, 128, 128), jnp.bfloat16)
        if earlier
        else (sums, peaks),
        in_specs=[vmem] * (1 + len(packs) + len(earlier)),
        out_specs=vmem if earlier else (vmem, vmem),
        scratch_shapes=scratch,
        name="attend_rest" if earlier else "attend_first",
    )(q, *packs, *earlier)


def stack_kernel(first, second, out, arrived):
    rows = first.shape[0]
    copies = [
        pltpu.make_async_copy(first, out.at[pl.ds(0, rows)], arrived.at[0]),
        pltpu.make_async_copy(second, out.at[pl.ds(rows, second.shape[0])], arrived.at[1]),
    ]
    for copy in copies:
        copy.start()
    for copy in copies:
        copy.wait()


def stacked(first, second):
    anywhere = pl.BlockSpec(memory_space=pl.ANY)
    return pl.pallas_call(
        stack_kernel,
        out_shape=jax.ShapeDtypeStruct((2 * first.shape[0], first.shape[1]), first.dtype),
        in_specs=[anywhere, anywhere],
        out_specs=anywhere,
        scratch_shapes=[pltpu.SemaphoreType.DMA((2,))],
        name="stack_rows",
    )(first, second)


def expert_kernel(rows, gate, gate_far, up, up_far, down, down_far, out, joined, joined_down):
    sources, _, slots, width = rows.shape
    part = gate.shape[1]
    for n, piece in enumerate((gate, gate_far, up, up_far)):
        joined[n * part : (n + 1) * part, :] = piece[0]
    for n, piece in enumerate((down, down_far)):
        joined_down[n * part : (n + 1) * part, :] = piece[0]
    x = rows[...].reshape(sources * slots, width)
    values = lax.dot_general(
        x, joined[...], (((1,), (1,)), ((), ())), preferred_element_type=jnp.float32
    )
    gate_values = values[:, : 2 * part]
    active = gate_values / (1.0 + jnp.exp(-gate_values)) * values[:, 2 * part :]
    partial_value = jnp.dot(
        active.astype(jnp.bfloat16), joined_down[...], preferred_element_type=jnp.float32
    )
    out[...] = partial_value.astype(jnp.bfloat16).reshape(rows.shape)


def run_experts(rows, *weights):
    sources, experts, slots, width = rows.shape
    part = weights[0].shape[1]
    block = pl.BlockSpec((sources, 1, slots, width), lambda e: (0, e, 0, 0))
    weight = pl.BlockSpec((1, part, width), lambda e: (e, 0, 0))
    return pl.pallas_call(
        expert_kernel,
        grid=(experts,),
        out_shape=jax.ShapeDtypeStruct(rows.shape, jnp.bfloat16),
        in_specs=[block] + [weight] * len(weights),
        out_specs=block,
        scratch_shapes=[
            pltpu.VMEM((4 * part, width), jnp.bfloat16),
            pltpu.VMEM((2 * part, width), jnp.bfloat16),
        ],
        name="run_experts",
    )(rows, *weights)


def other_core(x):
    return lax.ppermute(x, "tp", [(i, i ^ 1) for i in range(lax.axis_size("tp"))])


def turned_ring(x, away):
    size = lax.axis_size("sp")
    return lax.ppermute(
        x,
        "sp",
        [(i, i // SEQ_SHARDS * SEQ_SHARDS + (i + away) % SEQ_SHARDS) for i in range(size)],
    )


def layer_norm(values, gain_vec, bias_vec):
    center = jnp.mean(values, axis=-1, keepdims=True)
    shifted = values - center
    variance = jnp.mean(shifted * shifted, axis=-1, keepdims=True)
    return (shifted * lax.rsqrt(variance + EPS_LAYER) * gain_vec + bias_vec).astype(jnp.bfloat16)


def local(
    residual,
    wide_query,
    narrow_query,
    wide_keys,
    narrow_keys,
    wide_values,
    narrow_values,
    wide_query_gain,
    wide_key_gain,
    narrow_query_gain,
    narrow_key_gain,
    wide_out,
    narrow_out,
    first_gain,
    first_bias,
    route_ids,
    route_weights,
    expert_gate,
    expert_up,
    expert_down,
    shared_gate,
    shared_up,
    shared_down,
    second_gain,
    second_bias,
):
    tp_size = lax.axis_size("tp")
    core_lines = [list(range(core, tp_size, 2)) for core in range(2)]
    out_weights = lax.all_gather(
        stacked(wide_out, narrow_out), "tp", axis=0, tiled=True, axis_index_groups=core_lines
    )
    rotated_queries, own_pack = prepare(
        wide_query.T,
        narrow_query.T,
        wide_keys,
        narrow_keys,
        wide_values,
        narrow_values,
        wide_query_gain,
        wide_key_gain,
        narrow_query_gain,
        narrow_key_gain,
    )
    packs = [own_pack] + [turned_ring(own_pack, away) for away in range(1, SEQ_SHARDS)]
    earlier = attend(rotated_queries, packs[:2])
    mixed = attend(rotated_queries, packs[2:], earlier)
    tokens = lax.all_to_all(
        mixed, "tp", split_axis=0, concat_axis=0, tiled=True, axis_index_groups=core_lines
    ).reshape(out_weights.shape[0], 128)
    half = residual.shape[0]
    core = lax.axis_index("tp") % 2
    own_tokens = lax.dynamic_slice_in_dim(tokens, core * half, half, 1)
    far_tokens = lax.dynamic_slice_in_dim(tokens, (1 - core) * half, half, 1)
    heads_first = (((0,), (0,)), ((), ()))
    far_part = lax.dot_general(
        far_tokens, out_weights, heads_first, preferred_element_type=jnp.float32
    )
    own_part = lax.dot_general(
        own_tokens, out_weights, heads_first, preferred_element_type=jnp.float32
    )
    projected = own_part + other_core(far_part)
    hidden = layer_norm(ALPHA * residual.astype(jnp.float32) + projected, first_gain, first_bias)
    device_rows = hidden.shape[0]
    model_width = hidden.shape[1]
    sp_size = lax.axis_size("sp")
    top_count = route_ids.shape[1]
    experts = LOCAL_EXPERTS * sp_size
    capacity = max(2, (5 * device_rows * top_count + 4 * experts - 1) // (4 * experts))
    flat_ids = route_ids.reshape(-1)
    expert_hits = (flat_ids[:, None] == jnp.arange(experts, dtype=jnp.int32)[None, :]).astype(
        jnp.int32
    )
    earlier = jnp.sum((jnp.cumsum(expert_hits, axis=0) - expert_hits) * expert_hits, axis=1)
    slot_index = flat_ids * capacity + earlier
    chosen = (
        slot_index[:, None] == jnp.arange(experts * capacity, dtype=jnp.int32)[None, :]
    ).astype(jnp.float32)
    chosen = chosen.reshape(device_rows, top_count, experts * capacity)
    placing = jnp.sum(chosen, axis=1).astype(jnp.bfloat16)
    mixing = jnp.sum(chosen * route_weights[:, :, None], axis=1)
    outgoing = jnp.einsum("rs,rd->sd", placing, hidden, preferred_element_type=jnp.float32).astype(
        jnp.bfloat16
    )
    outgoing = outgoing.reshape(sp_size, LOCAL_EXPERTS, capacity, model_width)
    arrived = lax.all_to_all(outgoing, "sp", split_axis=0, concat_axis=0, tiled=True)
    slab = jnp.transpose(arrived, (1, 2, 0, 3)).reshape(
        LOCAL_EXPERTS, capacity * sp_size, model_width
    )
    piece_rows = lax.all_gather(slab, "tp", axis=0, tiled=False, axis_index_groups=core_lines)
    gate_rows = jnp.transpose(expert_gate, (0, 2, 1))
    up_rows = jnp.transpose(expert_up, (0, 2, 1))
    partial_value = run_experts(
        piece_rows,
        gate_rows,
        other_core(gate_rows),
        up_rows,
        other_core(up_rows),
        expert_down,
        other_core(expert_down),
    )
    summed = lax.psum_scatter(
        partial_value, "tp", scatter_dimension=0, tiled=False, axis_index_groups=core_lines
    )
    summed = summed.reshape(LOCAL_EXPERTS, capacity, sp_size, model_width)
    returned = lax.all_to_all(
        jnp.transpose(summed, (2, 0, 1, 3)), "sp", split_axis=0, concat_axis=0, tiled=True
    )
    routed = jnp.dot(mixing, returned.reshape(-1, model_width).astype(jnp.float32))
    shared_gate_values = jnp.dot(hidden, shared_gate, preferred_element_type=jnp.float32)
    shared_up_values = jnp.dot(hidden, shared_up, preferred_element_type=jnp.float32)
    shared_active = (jax.nn.silu(shared_gate_values) * shared_up_values).astype(jnp.bfloat16)
    shared_output = jnp.dot(shared_active, shared_down, preferred_element_type=jnp.float32)
    base = lax.optimization_barrier(ALPHA * hidden.astype(jnp.float32) + shared_output)
    return layer_norm(base + routed, second_gain, second_bias)


def solution(mesh):
    in_specs = (
        P(("sp", "tp"), None),
        P("sp", "tp"),
        P("sp", "tp"),
        P("sp", None),
        P("sp", None),
        P("sp", None),
        P("sp", None),
        P(),
        P(),
        P(),
        P(),
        P("tp", None),
        P("tp", None),
        P(),
        P(),
        P(("sp", "tp"), None),
        P(("sp", "tp"), None),
        P("sp", None, "tp"),
        P("sp", None, "tp"),
        P("sp", "tp", None),
        P(),
        P(),
        P(),
        P(),
        P(),
    )
    out_specs = P(("sp", "tp"), None)
    return jax.shard_map(local, mesh=mesh, in_specs=in_specs, out_specs=out_specs, check_vma=False)
```

```python
import functools

import jax
import jax.numpy as jnp
from jax import lax
from jax.experimental import pallas as pl
from jax.experimental.pallas import tpu as pltpu
from jax.sharding import PartitionSpec as P

LOCAL_EXPERTS = 2
EPS_LAYER = 1e-05
ALPHA = 2.0**0.25
EPS_HEAD = 1e-06
THETA = 10000.0
GRID_WIDTH = 64
SEQ_SHARDS = 4
LOG2E = 1.4426950408889634
WIDE_SIZE = 64
NARROW_SIZE = 32
KEY_ROWS = WIDE_SIZE + NARROW_SIZE
ONES_ROWS = 16
BLOCK_Q = 256
CHUNK = 512


def column(ref):
    size = ref.shape[1]
    spread = jnp.broadcast_to(ref[...], (size, size))
    diagonal = lax.broadcasted_iota(jnp.int32, (size, size), 0) == lax.broadcasted_iota(
        jnp.int32, (size, size), 1
    )
    return jnp.sum(jnp.where(diagonal, spread, 0.0), axis=1, keepdims=True)


def normed(heads, gain):
    mean_square = jnp.mean(heads * heads, axis=0, keepdims=True)
    return heads * lax.rsqrt(mean_square + EPS_HEAD) * gain


def turned(heads, tables):
    n = heads.shape[0] // 4
    parts = []
    for half, (cosine, sine) in enumerate(tables):
        a = heads[2 * half * n : (2 * half + 1) * n]
        b = heads[(2 * half + 1) * n : (2 * half + 2) * n]
        parts += [a * cosine - b * sine, b * cosine + a * sine]
    return jnp.concatenate(parts, axis=0)


def angle_tables(quarter, first_row, tokens):
    frequency = jnp.exp(
        lax.broadcasted_iota(jnp.int32, (quarter, tokens), 0).astype(jnp.float32)
        * (-jnp.log(jnp.float32(THETA)) / quarter)
    )
    token = lax.broadcasted_iota(jnp.int32, (quarter, tokens), 1)
    row_angle = (token // GRID_WIDTH + first_row).astype(jnp.float32) * frequency
    col_angle = (token % GRID_WIDTH).astype(jnp.float32) * frequency
    return ((jnp.cos(row_angle), jnp.sin(row_angle)), (jnp.cos(col_angle), jnp.sin(col_angle)))


def prepare_kernel(wqt, nqt, wk, nk, wv, nv, wqg, wkg, nqg, nkg, q_out, kv_out, turn):
    tokens = wqt.shape[1]
    tp = lax.axis_index("tp")
    first_row = lax.axis_index("sp") % SEQ_SHARDS * (tokens // GRID_WIDTH)
    wide_tables = angle_tables(WIDE_SIZE // 4, first_row, tokens)
    narrow_tables = angle_tables(NARROW_SIZE // 4, first_row, tokens)

    def picked(ref, start, size):
        block = start // 128
        columns = ref[:, pl.ds(pl.multiple_of(block * 128, 128), 128)]
        turn[...] = columns.astype(jnp.float32).T
        return turn[pl.ds(pl.multiple_of(start % 128, size), size), :]

    wide_start = tp // 4 * WIDE_SIZE
    narrow_start = tp // 2 * NARROW_SIZE
    keys = turned(normed(picked(wk, wide_start, WIDE_SIZE), column(wkg)), wide_tables)
    kv_out[0:64, :] = keys.astype(jnp.bfloat16)
    keys = turned(normed(picked(nk, narrow_start, NARROW_SIZE), column(nkg)), narrow_tables)
    kv_out[64:96, :] = keys.astype(jnp.bfloat16)
    kv_out[96:160, :] = picked(wv, wide_start, WIDE_SIZE).astype(jnp.bfloat16)
    kv_out[160:192, :] = picked(nv, narrow_start, NARROW_SIZE).astype(jnp.bfloat16)
    wide = turned(normed(wqt[...].astype(jnp.float32), column(wqg)), wide_tables)
    q_out[0:64, 0:tokens] = wide.astype(jnp.bfloat16)
    q_out[64:128, 0:tokens] = jnp.zeros((64, tokens), jnp.bfloat16)
    q_out[0:64, tokens:] = jnp.zeros((64, 2 * tokens), jnp.bfloat16)
    q_out[96:128, tokens:] = jnp.zeros((32, 2 * tokens), jnp.bfloat16)
    for head in range(2):
        rows = nqt[NARROW_SIZE * head : NARROW_SIZE * (head + 1), :].astype(jnp.float32)
        narrow = turned(normed(rows, column(nqg)), narrow_tables)
        q_out[64:96, tokens * (head + 1) : tokens * (head + 2)] = narrow.astype(jnp.bfloat16)


def prepare(wqt, nqt, wk, nk, wv, nv, wqg, wkg, nqg, nkg):
    tokens = wqt.shape[1]
    vmem = pl.BlockSpec(memory_space=pltpu.VMEM)
    return pl.pallas_call(
        prepare_kernel,
        out_shape=(
            jax.ShapeDtypeStruct((128, 3 * tokens), jnp.bfloat16),
            jax.ShapeDtypeStruct((192, tokens), jnp.bfloat16),
        ),
        in_specs=[vmem] * 10,
        out_specs=(vmem, vmem),
        scratch_shapes=[pltpu.VMEM((128, tokens), jnp.float32)],
        name="prepare_heads",
    )(
        wqt, nqt, wk, nk, wv, nv,
        wqg.reshape(1, -1), wkg.reshape(1, -1), nqg.reshape(1, -1), nkg.reshape(1, -1),
    )


def attend_kernel(*refs, pieces, resumed):
    q = refs[0]
    packs = refs[1 : 1 + pieces]
    refs = refs[1 + pieces :]
    if resumed:
        before, peak_before, out, keys, values, scores0, scores1, mixed = refs
    else:
        sums, peaks, keys, values, scores0, scores1 = refs
    tokens = packs[0].shape[1]
    total = pieces * tokens
    blocks = q.shape[1] // BLOCK_Q
    wide_blocks = tokens // BLOCK_Q
    values[KEY_ROWS:, :] = jnp.ones((ONES_ROWS, total), jnp.bfloat16)
    for n, kv in enumerate(packs):
        piece = kv[0:KEY_ROWS, :].astype(jnp.float32)
        padded = jnp.concatenate([piece, jnp.zeros((128 - KEY_ROWS, tokens), jnp.float32)], axis=0)
        keys[n * tokens : (n + 1) * tokens, :] = padded.T.astype(jnp.bfloat16)
        values[0:KEY_ROWS, n * tokens : (n + 1) * tokens] = kv[KEY_ROWS:, :]

    def scored(c, query, into, largest):
        part = jnp.dot(
            keys[c * CHUNK : (c + 1) * CHUNK, :], query, preferred_element_type=jnp.float32
        )
        into[c * CHUNK : (c + 1) * CHUNK, :] = part
        return jnp.maximum(largest, jnp.max(part.reshape(CHUNK // 8, 8, BLOCK_Q), axis=0))

    lowest = jnp.full((8, BLOCK_Q), -jnp.inf, jnp.float32)
    query_at = lambda b: q[:, pl.ds(pl.multiple_of(b * BLOCK_Q, BLOCK_Q), BLOCK_Q)]

    def step(b, current, following, largest):
        query = query_at(jnp.minimum(b + 1, blocks - 1))
        peak = jnp.max(largest, axis=0, keepdims=True)
        factor = jnp.where(
            b < wide_blocks,
            jnp.float32(WIDE_SIZE**-0.5 * LOG2E),
            jnp.float32(NARROW_SIZE**-0.5 * LOG2E),
        )
        if resumed:
            earlier = peak_before[b][0:1]
            peak = jnp.maximum(peak, earlier)
            total_mixed = before[b] * jnp.exp2((earlier - peak) * factor)
        else:
            total_mixed = jnp.zeros((KEY_ROWS + ONES_ROWS, BLOCK_Q), jnp.float32)
        next_largest = lowest
        for c in range(total // CHUNK):
            next_largest = scored(c, query, following, next_largest)
            raw = current[c * CHUNK : (c + 1) * CHUNK, :]
            weights = jnp.exp2((raw - peak) * factor).astype(jnp.bfloat16)
            total_mixed = total_mixed + jnp.dot(
                values[:, c * CHUNK : (c + 1) * CHUNK], weights, preferred_element_type=jnp.float32
            )
        if resumed:
            mixed[b] = total_mixed[:KEY_ROWS] / total_mixed[KEY_ROWS : KEY_ROWS + 1]
        else:
            sums[b] = total_mixed
            peaks[b] = jnp.broadcast_to(peak, (8, BLOCK_Q))
        return next_largest

    largest = lowest
    first = query_at(0)
    for c in range(total // CHUNK):
        largest = scored(c, first, scores0, largest)

    def pair(i, largest):
        largest = step(2 * i, scores0, scores1, largest)
        return step(2 * i + 1, scores1, scores0, largest)

    lax.fori_loop(0, blocks // 2, pair, largest)
    if not resumed:
        return
    for b in range(wide_blocks):
        rows = jnp.concatenate(
            [
                mixed[b, 0:WIDE_SIZE],
                mixed[wide_blocks + b, WIDE_SIZE:KEY_ROWS],
                mixed[2 * wide_blocks + b, WIDE_SIZE:KEY_ROWS],
            ],
            axis=0,
        )
        out[b * BLOCK_Q : (b + 1) * BLOCK_Q, :] = rows.T.astype(jnp.bfloat16)


def attend(q, packs, earlier=()):
    tokens = packs[0].shape[1]
    total = len(packs) * tokens
    blocks = q.shape[1] // BLOCK_Q
    sums = jax.ShapeDtypeStruct((blocks, KEY_ROWS + ONES_ROWS, BLOCK_Q), jnp.float32)
    peaks = jax.ShapeDtypeStruct((blocks, 8, BLOCK_Q), jnp.float32)
    vmem = pl.BlockSpec(memory_space=pltpu.VMEM)
    scratch = [
        pltpu.VMEM((total, 128), jnp.bfloat16),
        pltpu.VMEM((KEY_ROWS + ONES_ROWS, total), jnp.bfloat16),
        pltpu.VMEM((total, BLOCK_Q), jnp.float32),
        pltpu.VMEM((total, BLOCK_Q), jnp.float32),
    ]
    if earlier:
        scratch.append(pltpu.VMEM((blocks, KEY_ROWS, BLOCK_Q), jnp.float32))
    return pl.pallas_call(
        functools.partial(attend_kernel, pieces=len(packs), resumed=bool(earlier)),
        out_shape=jax.ShapeDtypeStruct((tokens, 128), jnp.bfloat16) if earlier else (sums, peaks),
        in_specs=[vmem] * (1 + len(packs) + len(earlier)),
        out_specs=vmem if earlier else (vmem, vmem),
        scratch_shapes=scratch,
        name="attend_rest" if earlier else "attend_first",
    )(q, *packs, *earlier)


def stack_kernel(first, second, out):
    out[: first.shape[0]] = first[...]
    out[first.shape[0] :] = second[...]


def stacked(first, second):
    vmem = pl.BlockSpec(memory_space=pltpu.VMEM)
    return pl.pallas_call(
        stack_kernel,
        out_shape=jax.ShapeDtypeStruct((2 * first.shape[0], first.shape[1]), first.dtype),
        in_specs=[vmem, vmem],
        out_specs=vmem,
        name="stack_rows",
    )(first, second)


def expert_kernel(*refs, expert):
    rows, gate, gate_far, up, up_far, down, down_far = refs[:7]
    out = refs[-1]
    sources, _, slots, width = out.shape
    x = rows[...].reshape(sources * slots, width)
    along = (((1,), (1,)), ((), ()))
    partial_value = jnp.zeros((sources * slots, width), jnp.float32)
    if expert:
        count = sources * slots
        place = lax.broadcasted_iota(jnp.int32, (count, 1), 0)
        source, slot, shard = place // slots, place % slots // 16, place % 16
        wanted = shard * (count // 16) + source * (slots // 16) + slot
        order = (wanted == lax.broadcasted_iota(jnp.int32, (count, count), 1)).astype(jnp.bfloat16)
    for g, u, d in ((gate, up, down), (gate_far, up_far, down_far)):
        gate_values = lax.dot_general(x, g[0], along, preferred_element_type=jnp.float32)
        up_values = lax.dot_general(x, u[0], along, preferred_element_type=jnp.float32)
        active = gate_values / (1.0 + jnp.exp(-gate_values)) * up_values
        active = active.astype(jnp.bfloat16)
        if expert:
            active = jnp.dot(order, active, preferred_element_type=jnp.float32)
            active = active.astype(jnp.bfloat16)
        partial_value = partial_value + jnp.dot(active, d[0], preferred_element_type=jnp.float32)
    out[...] = partial_value.astype(jnp.bfloat16).reshape(out.shape)


def run_expert(expert, rows, weights, shape, written=None):
    sources, _, slots, width = shape
    whole = pl.BlockSpec(rows.shape, lambda i: (0, 0, 0))
    weight = pl.BlockSpec((1, *weights[0].shape[1:]), lambda i: (expert, 0, 0))
    block = pl.BlockSpec((sources, 1, slots, width), lambda i: (0, expert, 0, 0))
    kept = [] if written is None else [written]
    return pl.pallas_call(
        functools.partial(expert_kernel, expert=expert),
        grid=(1,),
        out_shape=jax.ShapeDtypeStruct(shape, jnp.bfloat16),
        in_specs=[whole] + [weight] * 6 + [pl.BlockSpec(memory_space=pl.ANY)] * len(kept),
        out_specs=block,
        input_output_aliases={7: 0} if kept else {},
        name=f"run_expert_{expert}",
    )(rows, *weights, *kept)


def other_core(x):
    return lax.ppermute(x, "tp", [(i, i ^ 1) for i in range(lax.axis_size("tp"))])


def turned_ring(x, away):
    size = lax.axis_size("sp")
    return lax.ppermute(
        x,
        "sp",
        [(i, i // SEQ_SHARDS * SEQ_SHARDS + (i + away) % SEQ_SHARDS) for i in range(size)],
    )


def layer_norm(values, gain_vec, bias_vec):
    center = jnp.mean(values, axis=-1, keepdims=True)
    shifted = values - center
    variance = jnp.mean(shifted * shifted, axis=-1, keepdims=True)
    return (shifted * lax.rsqrt(variance + EPS_LAYER) * gain_vec + bias_vec).astype(jnp.bfloat16)


def local(
    residual,
    wide_query,
    narrow_query,
    wide_keys,
    narrow_keys,
    wide_values,
    narrow_values,
    wide_query_gain,
    wide_key_gain,
    narrow_query_gain,
    narrow_key_gain,
    wide_out,
    narrow_out,
    first_gain,
    first_bias,
    route_ids,
    route_weights,
    expert_gate,
    expert_up,
    expert_down,
    shared_gate,
    shared_up,
    shared_down,
    second_gain,
    second_bias,
):
    tp_size = lax.axis_size("tp")
    out_weights = lax.all_gather(
        stacked(wide_out, narrow_out), "tp", axis=0, tiled=True
    )
    rotated_queries, own_pack = prepare(
        wide_query.T,
        narrow_query.T,
        wide_keys,
        narrow_keys,
        wide_values,
        narrow_values,
        wide_query_gain,
        wide_key_gain,
        narrow_query_gain,
        narrow_key_gain,
    )
    packs = [own_pack] + [turned_ring(own_pack, away) for away in range(1, SEQ_SHARDS)]
    earlier = attend(rotated_queries, packs[:2])
    mixed = attend(rotated_queries, packs[2:], earlier)
    tokens = lax.all_to_all(mixed, "tp", split_axis=0, concat_axis=1, tiled=True)
    projected = jnp.dot(tokens, out_weights, preferred_element_type=jnp.float32)
    hidden = layer_norm(ALPHA * residual.astype(jnp.float32) + projected, first_gain, first_bias)
    device_rows = hidden.shape[0]
    model_width = hidden.shape[1]
    sp_size = lax.axis_size("sp")
    top_count = route_ids.shape[1]
    experts = LOCAL_EXPERTS * sp_size
    capacity = max(2, (5 * device_rows * top_count + 4 * experts - 1) // (4 * experts))
    flat_ids = route_ids.reshape(-1)
    expert_hits = (flat_ids[:, None] == jnp.arange(experts, dtype=jnp.int32)[None, :]).astype(
        jnp.int32
    )
    earlier = jnp.sum((jnp.cumsum(expert_hits, axis=0) - expert_hits) * expert_hits, axis=1)
    slot_index = flat_ids * capacity + earlier
    chosen = (
        slot_index[:, None] == jnp.arange(experts * capacity, dtype=jnp.int32)[None, :]
    ).astype(jnp.float32)
    chosen = chosen.reshape(device_rows, top_count, experts * capacity)
    placing = jnp.sum(chosen, axis=1).astype(jnp.bfloat16)
    placing = placing.reshape(device_rows, sp_size, LOCAL_EXPERTS, capacity)
    placing = placing[:, :, 0].reshape(device_rows, sp_size * capacity)
    line_place = lax.axis_index("tp") // 2
    lines = tp_size // 2
    slot_of = (flat_ids // 2 * lines + line_place) * capacity + earlier
    target = jnp.where(flat_ids % 2 == 1, slot_of, -1).reshape(device_rows, top_count)
    mixing = jnp.sum(chosen * route_weights[:, :, None], axis=1)
    core_lines = [list(range(core, tp_size, 2)) for core in range(2)]
    line_hidden = lax.all_gather(hidden, "tp", axis=0, tiled=True, axis_index_groups=core_lines)
    targets = lax.all_gather(
        target.astype(jnp.float32), "tp", axis=0, tiled=True, axis_index_groups=core_lines
    )
    outgoing = jnp.einsum("rs,rd->sd", placing, hidden, preferred_element_type=jnp.float32).astype(
        jnp.bfloat16
    )
    outgoing = outgoing.reshape(sp_size, capacity, model_width)
    arrived = lax.all_to_all(outgoing, "sp", split_axis=0, concat_axis=0, tiled=True)
    slab = jnp.transpose(arrived, (1, 0, 2)).reshape(capacity * sp_size, model_width)
    first_rows = lax.all_gather(slab, "tp", axis=0, tiled=False, axis_index_groups=core_lines)
    slots = sp_size * lines * capacity
    picking = jnp.sum(
        (targets[:, :, None] == jnp.arange(slots, dtype=jnp.float32)).astype(jnp.float32), axis=1
    ).astype(jnp.bfloat16)
    leaving = lax.dot_general(
        picking, line_hidden, (((0,), (0,)), ((), ())), preferred_element_type=jnp.float32
    ).astype(jnp.bfloat16)
    second_rows = lax.all_to_all(
        leaving.reshape(sp_size, lines * capacity, model_width),
        "sp",
        split_axis=0,
        concat_axis=0,
        tiled=True,
    )
    gate_rows = jnp.transpose(expert_gate, (0, 2, 1))
    up_rows = jnp.transpose(expert_up, (0, 2, 1))
    weights = (
        gate_rows,
        other_core(gate_rows),
        up_rows,
        other_core(up_rows),
        expert_down,
        other_core(expert_down),
    )
    shape = (lines, LOCAL_EXPERTS, capacity * sp_size, model_width)
    partial_value = run_expert(0, first_rows, weights, shape)
    partial_value = run_expert(1, second_rows, weights, shape, partial_value)
    summed = lax.psum_scatter(
        partial_value, "tp", scatter_dimension=0, tiled=False, axis_index_groups=core_lines
    )
    summed = summed.reshape(LOCAL_EXPERTS, capacity, sp_size, model_width)
    returned = lax.all_to_all(
        jnp.transpose(summed, (2, 0, 1, 3)), "sp", split_axis=0, concat_axis=0, tiled=True
    )
    routed = jnp.dot(mixing, returned.reshape(-1, model_width).astype(jnp.float32))
    shared_gate_values = jnp.dot(hidden, shared_gate, preferred_element_type=jnp.float32)
    shared_up_values = jnp.dot(hidden, shared_up, preferred_element_type=jnp.float32)
    shared_active = (jax.nn.silu(shared_gate_values) * shared_up_values).astype(jnp.bfloat16)
    shared_output = jnp.dot(shared_active, shared_down, preferred_element_type=jnp.float32)
    base = lax.optimization_barrier(ALPHA * hidden.astype(jnp.float32) + shared_output)
    return layer_norm(base + routed, second_gain, second_bias)


def solution(mesh):
    in_specs = (
        P(("sp", "tp"), None),
        P("sp", "tp"),
        P("sp", "tp"),
        P("sp", None),
        P("sp", None),
        P("sp", None),
        P("sp", None),
        P(),
        P(),
        P(),
        P(),
        P("tp", None),
        P("tp", None),
        P(),
        P(),
        P(("sp", "tp"), None),
        P(("sp", "tp"), None),
        P("sp", None, "tp"),
        P("sp", None, "tp"),
        P("sp", "tp", None),
        P(),
        P(),
        P(),
        P(),
        P(),
    )
    out_specs = P(("sp", "tp"), None)
    return jax.shard_map(local, mesh=mesh, in_specs=in_specs, out_specs=out_specs, check_vma=False)
```

```python
import functools

import jax
import jax.numpy as jnp
from jax import lax
from jax.experimental import pallas as pl
from jax.experimental.pallas import tpu as pltpu
from jax.sharding import PartitionSpec as P

LOCAL_EXPERTS = 2
EPS_LAYER = 1e-05
ALPHA = 2.0**0.25
EPS_HEAD = 1e-06
THETA = 10000.0
GRID_WIDTH = 64
SEQ_SHARDS = 4
LOG2E = 1.4426950408889634
WIDE_SIZE = 64
NARROW_SIZE = 32
KEY_ROWS = WIDE_SIZE + NARROW_SIZE
ONES_ROWS = 16
BLOCK_Q = 256
CHUNK = 512


def column(ref):
    size = ref.shape[1]
    spread = jnp.broadcast_to(ref[...], (size, size))
    diagonal = lax.broadcasted_iota(jnp.int32, (size, size), 0) == lax.broadcasted_iota(
        jnp.int32, (size, size), 1
    )
    return jnp.sum(jnp.where(diagonal, spread, 0.0), axis=1, keepdims=True)


def normed(heads, gain):
    mean_square = jnp.mean(heads * heads, axis=0, keepdims=True)
    return heads * lax.rsqrt(mean_square + EPS_HEAD) * gain


def turned(heads, tables):
    n = heads.shape[0] // 4
    parts = []
    for half, (cosine, sine) in enumerate(tables):
        a = heads[2 * half * n : (2 * half + 1) * n]
        b = heads[(2 * half + 1) * n : (2 * half + 2) * n]
        parts += [a * cosine - b * sine, b * cosine + a * sine]
    return jnp.concatenate(parts, axis=0)


def angle_tables(quarter, first_row, tokens):
    frequency = jnp.exp(
        lax.broadcasted_iota(jnp.int32, (quarter, tokens), 0).astype(jnp.float32)
        * (-jnp.log(jnp.float32(THETA)) / quarter)
    )
    token = lax.broadcasted_iota(jnp.int32, (quarter, tokens), 1)
    row_angle = (token // GRID_WIDTH + first_row).astype(jnp.float32) * frequency
    col_angle = (token % GRID_WIDTH).astype(jnp.float32) * frequency
    return ((jnp.cos(row_angle), jnp.sin(row_angle)), (jnp.cos(col_angle), jnp.sin(col_angle)))


def prepare_kernel(wqt, nqt, wk, nk, wv, nv, wqg, wkg, nqg, nkg, q_out, kv_out, turn):
    tokens = wqt.shape[1]
    tp = lax.axis_index("tp")
    first_row = lax.axis_index("sp") % SEQ_SHARDS * (tokens // GRID_WIDTH)
    wide_tables = angle_tables(WIDE_SIZE // 4, first_row, tokens)
    narrow_tables = angle_tables(NARROW_SIZE // 4, first_row, tokens)

    def picked(ref, start, size):
        block = start // 128
        columns = ref[:, pl.ds(pl.multiple_of(block * 128, 128), 128)]
        turn[...] = columns.astype(jnp.float32).T
        return turn[pl.ds(pl.multiple_of(start % 128, size), size), :]

    wide_start = tp // 4 * WIDE_SIZE
    narrow_start = tp // 2 * NARROW_SIZE
    keys = turned(normed(picked(wk, wide_start, WIDE_SIZE), column(wkg)), wide_tables)
    kv_out[0:64, :] = keys.astype(jnp.bfloat16)
    keys = turned(normed(picked(nk, narrow_start, NARROW_SIZE), column(nkg)), narrow_tables)
    kv_out[64:96, :] = keys.astype(jnp.bfloat16)
    kv_out[96:160, :] = picked(wv, wide_start, WIDE_SIZE).astype(jnp.bfloat16)
    kv_out[160:192, :] = picked(nv, narrow_start, NARROW_SIZE).astype(jnp.bfloat16)
    wide = turned(normed(wqt[...].astype(jnp.float32), column(wqg)), wide_tables)
    q_out[0:64, 0:tokens] = wide.astype(jnp.bfloat16)
    q_out[64:128, 0:tokens] = jnp.zeros((64, tokens), jnp.bfloat16)
    q_out[0:64, tokens:] = jnp.zeros((64, 2 * tokens), jnp.bfloat16)
    q_out[96:128, tokens:] = jnp.zeros((32, 2 * tokens), jnp.bfloat16)
    for head in range(2):
        rows = nqt[NARROW_SIZE * head : NARROW_SIZE * (head + 1), :].astype(jnp.float32)
        narrow = turned(normed(rows, column(nqg)), narrow_tables)
        q_out[64:96, tokens * (head + 1) : tokens * (head + 2)] = narrow.astype(jnp.bfloat16)


def prepare(wqt, nqt, wk, nk, wv, nv, wqg, wkg, nqg, nkg):
    tokens = wqt.shape[1]
    vmem = pl.BlockSpec(memory_space=pltpu.VMEM)
    return pl.pallas_call(
        prepare_kernel,
        out_shape=(
            jax.ShapeDtypeStruct((128, 3 * tokens), jnp.bfloat16),
            jax.ShapeDtypeStruct((192, tokens), jnp.bfloat16),
        ),
        in_specs=[vmem] * 10,
        out_specs=(vmem, vmem),
        scratch_shapes=[pltpu.VMEM((128, tokens), jnp.float32)],
        name="prepare_heads",
    )(
        wqt, nqt, wk, nk, wv, nv,
        wqg.reshape(1, -1), wkg.reshape(1, -1), nqg.reshape(1, -1), nkg.reshape(1, -1),
    )


def attend_kernel(*refs, pieces, resumed):
    q = refs[0]
    packs = refs[1 : 1 + pieces]
    refs = refs[1 + pieces :]
    if resumed:
        before, peak_before, out, keys, values, scores0, scores1, mixed = refs
    else:
        sums, peaks, keys, values, scores0, scores1 = refs
    tokens = packs[0].shape[1]
    total = pieces * tokens
    blocks = q.shape[1] // BLOCK_Q
    wide_blocks = tokens // BLOCK_Q
    values[KEY_ROWS:, :] = jnp.ones((ONES_ROWS, total), jnp.bfloat16)
    for n, kv in enumerate(packs):
        piece = kv[0:KEY_ROWS, :].astype(jnp.float32)
        padded = jnp.concatenate([piece, jnp.zeros((128 - KEY_ROWS, tokens), jnp.float32)], axis=0)
        keys[n * tokens : (n + 1) * tokens, :] = padded.T.astype(jnp.bfloat16)
        values[0:KEY_ROWS, n * tokens : (n + 1) * tokens] = kv[KEY_ROWS:, :]

    def scored(c, query, into, largest):
        part = jnp.dot(
            keys[c * CHUNK : (c + 1) * CHUNK, :], query, preferred_element_type=jnp.float32
        )
        into[c * CHUNK : (c + 1) * CHUNK, :] = part
        return jnp.maximum(largest, jnp.max(part.reshape(CHUNK // 8, 8, BLOCK_Q), axis=0))

    lowest = jnp.full((8, BLOCK_Q), -jnp.inf, jnp.float32)
    query_at = lambda b: q[:, pl.ds(pl.multiple_of(b * BLOCK_Q, BLOCK_Q), BLOCK_Q)]

    def step(b, current, following, largest):
        query = query_at(jnp.minimum(b + 1, blocks - 1))
        peak = jnp.max(largest, axis=0, keepdims=True)
        factor = jnp.where(
            b < wide_blocks,
            jnp.float32(WIDE_SIZE**-0.5 * LOG2E),
            jnp.float32(NARROW_SIZE**-0.5 * LOG2E),
        )
        if resumed:
            earlier = peak_before[b][0:1]
            peak = jnp.maximum(peak, earlier)
            total_mixed = before[b] * jnp.exp2((earlier - peak) * factor)
        else:
            total_mixed = jnp.zeros((KEY_ROWS + ONES_ROWS, BLOCK_Q), jnp.float32)
        next_largest = lowest
        for c in range(total // CHUNK):
            next_largest = scored(c, query, following, next_largest)
            raw = current[c * CHUNK : (c + 1) * CHUNK, :]
            weights = jnp.exp2((raw - peak) * factor).astype(jnp.bfloat16)
            total_mixed = total_mixed + jnp.dot(
                values[:, c * CHUNK : (c + 1) * CHUNK], weights, preferred_element_type=jnp.float32
            )
        if resumed:
            mixed[b] = total_mixed[:KEY_ROWS] / total_mixed[KEY_ROWS : KEY_ROWS + 1]
        else:
            sums[b] = total_mixed
            peaks[b] = jnp.broadcast_to(peak, (8, BLOCK_Q))
        return next_largest

    largest = lowest
    first = query_at(0)
    for c in range(total // CHUNK):
        largest = scored(c, first, scores0, largest)

    def pair(i, largest):
        largest = step(2 * i, scores0, scores1, largest)
        return step(2 * i + 1, scores1, scores0, largest)

    lax.fori_loop(0, blocks // 2, pair, largest)
    if not resumed:
        return
    for b in range(wide_blocks):
        rows = jnp.concatenate(
            [
                mixed[b, 0:WIDE_SIZE],
                mixed[wide_blocks + b, WIDE_SIZE:KEY_ROWS],
                mixed[2 * wide_blocks + b, WIDE_SIZE:KEY_ROWS],
            ],
            axis=0,
        )
        out[b * BLOCK_Q : (b + 1) * BLOCK_Q, :] = rows.T.astype(jnp.bfloat16)


def attend(q, packs, earlier=()):
    tokens = packs[0].shape[1]
    total = len(packs) * tokens
    blocks = q.shape[1] // BLOCK_Q
    sums = jax.ShapeDtypeStruct((blocks, KEY_ROWS + ONES_ROWS, BLOCK_Q), jnp.float32)
    peaks = jax.ShapeDtypeStruct((blocks, 8, BLOCK_Q), jnp.float32)
    vmem = pl.BlockSpec(memory_space=pltpu.VMEM)
    scratch = [
        pltpu.VMEM((total, 128), jnp.bfloat16),
        pltpu.VMEM((KEY_ROWS + ONES_ROWS, total), jnp.bfloat16),
        pltpu.VMEM((total, BLOCK_Q), jnp.float32),
        pltpu.VMEM((total, BLOCK_Q), jnp.float32),
    ]
    if earlier:
        scratch.append(pltpu.VMEM((blocks, KEY_ROWS, BLOCK_Q), jnp.float32))
    return pl.pallas_call(
        functools.partial(attend_kernel, pieces=len(packs), resumed=bool(earlier)),
        out_shape=jax.ShapeDtypeStruct((tokens, 128), jnp.bfloat16) if earlier else (sums, peaks),
        in_specs=[vmem] * (1 + len(packs) + len(earlier)),
        out_specs=vmem if earlier else (vmem, vmem),
        scratch_shapes=scratch,
        name="attend_rest" if earlier else "attend_first",
    )(q, *packs, *earlier)


def stack_kernel(first, second, out):
    out[: first.shape[0]] = first[...]
    out[first.shape[0] :] = second[...]


def stacked(first, second):
    vmem = pl.BlockSpec(memory_space=pltpu.VMEM)
    return pl.pallas_call(
        stack_kernel,
        out_shape=jax.ShapeDtypeStruct((2 * first.shape[0], first.shape[1]), first.dtype),
        in_specs=[vmem, vmem],
        out_specs=vmem,
        name="stack_rows",
    )(first, second)


def expert_kernel(rows, gate, gate_far, up, up_far, down, down_far, out):
    sources, _, slots, width = rows.shape
    x = rows[...].reshape(sources * slots, width)
    along = (((1,), (1,)), ((), ()))
    partial_value = jnp.zeros(x.shape, jnp.float32)
    for g, u, d in ((gate, up, down), (gate_far, up_far, down_far)):
        gate_values = lax.dot_general(x, g[0], along, preferred_element_type=jnp.float32)
        up_values = lax.dot_general(x, u[0], along, preferred_element_type=jnp.float32)
        active = gate_values / (1.0 + jnp.exp(-gate_values)) * up_values
        partial_value = partial_value + jnp.dot(
            active.astype(jnp.bfloat16), d[0], preferred_element_type=jnp.float32
        )
    out[...] = partial_value.astype(jnp.bfloat16).reshape(rows.shape)


def run_experts(rows, *weights):
    sources, experts, slots, width = rows.shape
    block = pl.BlockSpec((sources // 2, 1, slots, width), lambda e, r: (r, e, 0, 0))
    weight = pl.BlockSpec((1, *weights[0].shape[1:]), lambda e, r: (e, 0, 0))
    return pl.pallas_call(
        expert_kernel,
        grid=(experts, 2),
        out_shape=jax.ShapeDtypeStruct(rows.shape, jnp.bfloat16),
        in_specs=[block] + [weight] * len(weights),
        out_specs=block,
        name="run_experts",
    )(rows, *weights)


def other_core(x):
    return lax.ppermute(x, "tp", [(i, i ^ 1) for i in range(lax.axis_size("tp"))])


def turned_ring(x, away):
    size = lax.axis_size("sp")
    return lax.ppermute(
        x,
        "sp",
        [(i, i // SEQ_SHARDS * SEQ_SHARDS + (i + away) % SEQ_SHARDS) for i in range(size)],
    )


def layer_norm(values, gain_vec, bias_vec):
    center = jnp.mean(values, axis=-1, keepdims=True)
    shifted = values - center
    variance = jnp.mean(shifted * shifted, axis=-1, keepdims=True)
    return (shifted * lax.rsqrt(variance + EPS_LAYER) * gain_vec + bias_vec).astype(jnp.bfloat16)


def local(
    residual,
    wide_query,
    narrow_query,
    wide_keys,
    narrow_keys,
    wide_values,
    narrow_values,
    wide_query_gain,
    wide_key_gain,
    narrow_query_gain,
    narrow_key_gain,
    wide_out,
    narrow_out,
    first_gain,
    first_bias,
    route_ids,
    route_weights,
    expert_gate,
    expert_up,
    expert_down,
    shared_gate,
    shared_up,
    shared_down,
    second_gain,
    second_bias,
):
    tp_size = lax.axis_size("tp")
    out_weights = lax.all_gather(
        stacked(wide_out, narrow_out), "tp", axis=0, tiled=True
    )
    rotated_queries, own_pack = prepare(
        wide_query.T,
        narrow_query.T,
        wide_keys,
        narrow_keys,
        wide_values,
        narrow_values,
        wide_query_gain,
        wide_key_gain,
        narrow_query_gain,
        narrow_key_gain,
    )
    packs = [own_pack] + [turned_ring(own_pack, away) for away in range(1, SEQ_SHARDS)]
    earlier = attend(rotated_queries, packs[:2])
    mixed = attend(rotated_queries, packs[2:], earlier)
    tokens = lax.all_to_all(mixed, "tp", split_axis=0, concat_axis=1, tiled=True)
    projected = jnp.dot(tokens, out_weights, preferred_element_type=jnp.float32)
    hidden = layer_norm(ALPHA * residual.astype(jnp.float32) + projected, first_gain, first_bias)
    device_rows = hidden.shape[0]
    model_width = hidden.shape[1]
    sp_size = lax.axis_size("sp")
    top_count = route_ids.shape[1]
    experts = LOCAL_EXPERTS * sp_size
    capacity = max(2, (5 * device_rows * top_count + 4 * experts - 1) // (4 * experts))
    flat_ids = route_ids.reshape(-1)
    expert_hits = (flat_ids[:, None] == jnp.arange(experts, dtype=jnp.int32)[None, :]).astype(
        jnp.int32
    )
    earlier = jnp.sum((jnp.cumsum(expert_hits, axis=0) - expert_hits) * expert_hits, axis=1)
    slot_index = flat_ids * capacity + earlier
    chosen = (
        slot_index[:, None] == jnp.arange(experts * capacity, dtype=jnp.int32)[None, :]
    ).astype(jnp.float32)
    chosen = chosen.reshape(device_rows, top_count, experts * capacity)
    placing = jnp.sum(chosen, axis=1).astype(jnp.bfloat16)
    mixing = jnp.sum(chosen * route_weights[:, :, None], axis=1)
    outgoing = jnp.einsum("rs,rd->sd", placing, hidden, preferred_element_type=jnp.float32).astype(
        jnp.bfloat16
    )
    outgoing = outgoing.reshape(sp_size, LOCAL_EXPERTS, capacity, model_width)
    arrived = lax.all_to_all(outgoing, "sp", split_axis=0, concat_axis=0, tiled=True)
    slab = jnp.transpose(arrived, (1, 2, 0, 3)).reshape(
        LOCAL_EXPERTS, capacity * sp_size, model_width
    )
    core_lines = [list(range(core, tp_size, 2)) for core in range(2)]
    piece_rows = lax.all_gather(slab, "tp", axis=0, tiled=False, axis_index_groups=core_lines)
    gate_rows = jnp.transpose(expert_gate, (0, 2, 1))
    up_rows = jnp.transpose(expert_up, (0, 2, 1))
    partial_value = run_experts(
        piece_rows,
        gate_rows,
        other_core(gate_rows),
        up_rows,
        other_core(up_rows),
        expert_down,
        other_core(expert_down),
    )
    summed = lax.psum_scatter(
        partial_value, "tp", scatter_dimension=0, tiled=False, axis_index_groups=core_lines
    )
    summed = summed.reshape(LOCAL_EXPERTS, capacity, sp_size, model_width)
    returned = lax.all_to_all(
        jnp.transpose(summed, (2, 0, 1, 3)), "sp", split_axis=0, concat_axis=0, tiled=True
    )
    routed = jnp.dot(mixing, returned.reshape(-1, model_width).astype(jnp.float32))
    shared_gate_values = jnp.dot(hidden, shared_gate, preferred_element_type=jnp.float32)
    shared_up_values = jnp.dot(hidden, shared_up, preferred_element_type=jnp.float32)
    shared_active = (jax.nn.silu(shared_gate_values) * shared_up_values).astype(jnp.bfloat16)
    shared_output = jnp.dot(shared_active, shared_down, preferred_element_type=jnp.float32)
    base = lax.optimization_barrier(ALPHA * hidden.astype(jnp.float32) + shared_output)
    return layer_norm(base + routed, second_gain, second_bias)


def solution(mesh):
    in_specs = (
        P(("sp", "tp"), None),
        P("sp", "tp"),
        P("sp", "tp"),
        P("sp", None),
        P("sp", None),
        P("sp", None),
        P("sp", None),
        P(),
        P(),
        P(),
        P(),
        P("tp", None),
        P("tp", None),
        P(),
        P(),
        P(("sp", "tp"), None),
        P(("sp", "tp"), None),
        P("sp", None, "tp"),
        P("sp", None, "tp"),
        P("sp", "tp", None),
        P(),
        P(),
        P(),
        P(),
        P(),
    )
    out_specs = P(("sp", "tp"), None)
    return jax.shard_map(local, mesh=mesh, in_specs=in_specs, out_specs=out_specs, check_vma=False)
```

```python
import functools

import jax
import jax.numpy as jnp
from jax import lax
from jax.experimental import pallas as pl
from jax.experimental.pallas import tpu as pltpu
from jax.sharding import PartitionSpec as P

LOCAL_EXPERTS = 2
EPS_LAYER = 1e-05
ALPHA = 2.0**0.25
EPS_HEAD = 1e-06
THETA = 10000.0
GRID_WIDTH = 64
SEQ_SHARDS = 4
LOG2E = 1.4426950408889634
WIDE_SIZE = 64
NARROW_SIZE = 32
KEY_ROWS = WIDE_SIZE + NARROW_SIZE
ONES_ROWS = 16
BLOCK_Q = 256
CHUNK = 512


def column(ref):
    size = ref.shape[1]
    spread = jnp.broadcast_to(ref[...], (size, size))
    diagonal = lax.broadcasted_iota(jnp.int32, (size, size), 0) == lax.broadcasted_iota(
        jnp.int32, (size, size), 1
    )
    return jnp.sum(jnp.where(diagonal, spread, 0.0), axis=1, keepdims=True)


def normed(heads, gain):
    mean_square = jnp.mean(heads * heads, axis=0, keepdims=True)
    return heads * lax.rsqrt(mean_square + EPS_HEAD) * gain


def turned(heads, tables):
    n = heads.shape[0] // 4
    parts = []
    for half, (cosine, sine) in enumerate(tables):
        a = heads[2 * half * n : (2 * half + 1) * n]
        b = heads[(2 * half + 1) * n : (2 * half + 2) * n]
        parts += [a * cosine - b * sine, b * cosine + a * sine]
    return jnp.concatenate(parts, axis=0)


def angle_tables(quarter, first_row, tokens):
    frequency = jnp.exp(
        lax.broadcasted_iota(jnp.int32, (quarter, tokens), 0).astype(jnp.float32)
        * (-jnp.log(jnp.float32(THETA)) / quarter)
    )
    token = lax.broadcasted_iota(jnp.int32, (quarter, tokens), 1)
    row_angle = (token // GRID_WIDTH + first_row).astype(jnp.float32) * frequency
    col_angle = (token % GRID_WIDTH).astype(jnp.float32) * frequency
    return ((jnp.cos(row_angle), jnp.sin(row_angle)), (jnp.cos(col_angle), jnp.sin(col_angle)))


def prepare_kernel(wqt, nqt, wk, nk, wv, nv, wqg, wkg, nqg, nkg, q_out, kv_out, turn):
    tokens = wqt.shape[1]
    tp = lax.axis_index("tp")
    first_row = lax.axis_index("sp") % SEQ_SHARDS * (tokens // GRID_WIDTH)
    wide_tables = angle_tables(WIDE_SIZE // 4, first_row, tokens)
    narrow_tables = angle_tables(NARROW_SIZE // 4, first_row, tokens)

    def picked(ref, start, size):
        block = start // 128
        columns = ref[:, pl.ds(pl.multiple_of(block * 128, 128), 128)]
        turn[...] = columns.astype(jnp.float32).T
        return turn[pl.ds(pl.multiple_of(start % 128, size), size), :]

    wide_start = tp // 4 * WIDE_SIZE
    narrow_start = tp // 2 * NARROW_SIZE
    keys = turned(normed(picked(wk, wide_start, WIDE_SIZE), column(wkg)), wide_tables)
    kv_out[0:64, :] = keys.astype(jnp.bfloat16)
    keys = turned(normed(picked(nk, narrow_start, NARROW_SIZE), column(nkg)), narrow_tables)
    kv_out[64:96, :] = keys.astype(jnp.bfloat16)
    kv_out[96:160, :] = picked(wv, wide_start, WIDE_SIZE).astype(jnp.bfloat16)
    kv_out[160:192, :] = picked(nv, narrow_start, NARROW_SIZE).astype(jnp.bfloat16)
    wide = turned(normed(wqt[...].astype(jnp.float32), column(wqg)), wide_tables)
    q_out[0:64, 0:tokens] = wide.astype(jnp.bfloat16)
    q_out[64:128, 0:tokens] = jnp.zeros((64, tokens), jnp.bfloat16)
    q_out[0:64, tokens:] = jnp.zeros((64, 2 * tokens), jnp.bfloat16)
    q_out[96:128, tokens:] = jnp.zeros((32, 2 * tokens), jnp.bfloat16)
    for head in range(2):
        rows = nqt[NARROW_SIZE * head : NARROW_SIZE * (head + 1), :].astype(jnp.float32)
        narrow = turned(normed(rows, column(nqg)), narrow_tables)
        q_out[64:96, tokens * (head + 1) : tokens * (head + 2)] = narrow.astype(jnp.bfloat16)


def prepare(wqt, nqt, wk, nk, wv, nv, wqg, wkg, nqg, nkg):
    tokens = wqt.shape[1]
    vmem = pl.BlockSpec(memory_space=pltpu.VMEM)
    return pl.pallas_call(
        prepare_kernel,
        out_shape=(
            jax.ShapeDtypeStruct((128, 3 * tokens), jnp.bfloat16),
            jax.ShapeDtypeStruct((192, tokens), jnp.bfloat16),
        ),
        in_specs=[vmem] * 10,
        out_specs=(vmem, vmem),
        scratch_shapes=[pltpu.VMEM((128, tokens), jnp.float32)],
        name="prepare_heads",
    )(
        wqt, nqt, wk, nk, wv, nv,
        wqg.reshape(1, -1), wkg.reshape(1, -1), nqg.reshape(1, -1), nkg.reshape(1, -1),
    )


def attend_kernel(*refs, pieces, resumed):
    q = refs[0]
    packs = refs[1 : 1 + pieces]
    refs = refs[1 + pieces :]
    if resumed:
        before, peak_before, out, keys, values, scores0, scores1, mixed = refs
    else:
        sums, peaks, keys, values, scores0, scores1 = refs
    tokens = packs[0].shape[1]
    total = pieces * tokens
    blocks = q.shape[1] // BLOCK_Q
    wide_blocks = tokens // BLOCK_Q
    values[KEY_ROWS:, :] = jnp.ones((ONES_ROWS, total), jnp.bfloat16)
    for n, kv in enumerate(packs):
        piece = kv[0:KEY_ROWS, :].astype(jnp.float32)
        padded = jnp.concatenate([piece, jnp.zeros((128 - KEY_ROWS, tokens), jnp.float32)], axis=0)
        keys[n * tokens : (n + 1) * tokens, :] = padded.T.astype(jnp.bfloat16)
        values[0:KEY_ROWS, n * tokens : (n + 1) * tokens] = kv[KEY_ROWS:, :]

    def scored(c, query, into, largest):
        part = jnp.dot(
            keys[c * CHUNK : (c + 1) * CHUNK, :], query, preferred_element_type=jnp.float32
        )
        into[c * CHUNK : (c + 1) * CHUNK, :] = part
        return jnp.maximum(largest, jnp.max(part.reshape(CHUNK // 8, 8, BLOCK_Q), axis=0))

    lowest = jnp.full((8, BLOCK_Q), -jnp.inf, jnp.float32)
    query_at = lambda b: q[:, pl.ds(pl.multiple_of(b * BLOCK_Q, BLOCK_Q), BLOCK_Q)]

    def step(b, current, following, largest):
        query = query_at(jnp.minimum(b + 1, blocks - 1))
        peak = jnp.max(largest, axis=0, keepdims=True)
        factor = jnp.where(
            b < wide_blocks,
            jnp.float32(WIDE_SIZE**-0.5 * LOG2E),
            jnp.float32(NARROW_SIZE**-0.5 * LOG2E),
        )
        if resumed:
            earlier = peak_before[b][0:1]
            peak = jnp.maximum(peak, earlier)
            total_mixed = before[b] * jnp.exp2((earlier - peak) * factor)
        else:
            total_mixed = jnp.zeros((KEY_ROWS + ONES_ROWS, BLOCK_Q), jnp.float32)
        next_largest = lowest
        for c in range(total // CHUNK):
            next_largest = scored(c, query, following, next_largest)
            raw = current[c * CHUNK : (c + 1) * CHUNK, :]
            weights = jnp.exp2((raw - peak) * factor).astype(jnp.bfloat16)
            total_mixed = total_mixed + jnp.dot(
                values[:, c * CHUNK : (c + 1) * CHUNK], weights, preferred_element_type=jnp.float32
            )
        if resumed:
            mixed[b] = total_mixed[:KEY_ROWS] / total_mixed[KEY_ROWS : KEY_ROWS + 1]
        else:
            sums[b] = total_mixed
            peaks[b] = jnp.broadcast_to(peak, (8, BLOCK_Q))
        return next_largest

    largest = lowest
    first = query_at(0)
    for c in range(total // CHUNK):
        largest = scored(c, first, scores0, largest)

    def pair(i, largest):
        largest = step(2 * i, scores0, scores1, largest)
        return step(2 * i + 1, scores1, scores0, largest)

    lax.fori_loop(0, blocks // 2, pair, largest)
    if not resumed:
        return
    for b in range(wide_blocks):
        rows = jnp.concatenate(
            [
                mixed[b, 0:WIDE_SIZE],
                mixed[wide_blocks + b, WIDE_SIZE:KEY_ROWS],
                mixed[2 * wide_blocks + b, WIDE_SIZE:KEY_ROWS],
            ],
            axis=0,
        )
        out[b * BLOCK_Q : (b + 1) * BLOCK_Q, :] = rows.T.astype(jnp.bfloat16)


def attend(q, packs, earlier=()):
    tokens = packs[0].shape[1]
    total = len(packs) * tokens
    blocks = q.shape[1] // BLOCK_Q
    sums = jax.ShapeDtypeStruct((blocks, KEY_ROWS + ONES_ROWS, BLOCK_Q), jnp.float32)
    peaks = jax.ShapeDtypeStruct((blocks, 8, BLOCK_Q), jnp.float32)
    vmem = pl.BlockSpec(memory_space=pltpu.VMEM)
    scratch = [
        pltpu.VMEM((total, 128), jnp.bfloat16),
        pltpu.VMEM((KEY_ROWS + ONES_ROWS, total), jnp.bfloat16),
        pltpu.VMEM((total, BLOCK_Q), jnp.float32),
        pltpu.VMEM((total, BLOCK_Q), jnp.float32),
    ]
    if earlier:
        scratch.append(pltpu.VMEM((blocks, KEY_ROWS, BLOCK_Q), jnp.float32))
    return pl.pallas_call(
        functools.partial(attend_kernel, pieces=len(packs), resumed=bool(earlier)),
        out_shape=jax.ShapeDtypeStruct((tokens, 128), jnp.bfloat16) if earlier else (sums, peaks),
        in_specs=[vmem] * (1 + len(packs) + len(earlier)),
        out_specs=vmem if earlier else (vmem, vmem),
        scratch_shapes=scratch,
        name="attend_rest" if earlier else "attend_first",
    )(q, *packs, *earlier)


def stack_kernel(first, second, out):
    out[: first.shape[0]] = first[...]
    out[first.shape[0] :] = second[...]


def stacked(first, second):
    vmem = pl.BlockSpec(memory_space=pltpu.VMEM)
    return pl.pallas_call(
        stack_kernel,
        out_shape=jax.ShapeDtypeStruct((2 * first.shape[0], first.shape[1]), first.dtype),
        in_specs=[vmem, vmem],
        out_specs=vmem,
        name="stack_rows",
    )(first, second)


def expert_kernel(rows, gate, gate_far, up, up_far, down, down_far, out):
    sources, _, slots, width = rows.shape
    x = rows[...].reshape(sources * slots, width)
    along = (((1,), (1,)), ((), ()))
    partial_value = jnp.zeros(x.shape, jnp.float32)
    for g, u, d in ((gate, up, down), (gate_far, up_far, down_far)):
        gate_values = lax.dot_general(x, g[0], along, preferred_element_type=jnp.float32)
        up_values = lax.dot_general(x, u[0], along, preferred_element_type=jnp.float32)
        active = gate_values / (1.0 + jnp.exp(-gate_values)) * up_values
        partial_value = partial_value + jnp.dot(
            active.astype(jnp.bfloat16), d[0], preferred_element_type=jnp.float32
        )
    out[...] = partial_value.astype(jnp.bfloat16).reshape(rows.shape)


def run_experts(rows, *weights):
    sources, experts, slots, width = rows.shape
    block = pl.BlockSpec((sources, 1, slots, width), lambda e: (0, e, 0, 0))
    weight = pl.BlockSpec((1, *weights[0].shape[1:]), lambda e: (e, 0, 0))
    return pl.pallas_call(
        expert_kernel,
        grid=(experts,),
        out_shape=jax.ShapeDtypeStruct(rows.shape, jnp.bfloat16),
        in_specs=[block] + [weight] * len(weights),
        out_specs=block,
        name="run_experts",
    )(rows, *weights)


def other_core(x):
    return lax.ppermute(x, "tp", [(i, i ^ 1) for i in range(lax.axis_size("tp"))])


def turned_ring(x, away):
    size = lax.axis_size("sp")
    return lax.ppermute(
        x,
        "sp",
        [(i, i // SEQ_SHARDS * SEQ_SHARDS + (i + away) % SEQ_SHARDS) for i in range(size)],
    )


def layer_norm(values, gain_vec, bias_vec):
    center = jnp.mean(values, axis=-1, keepdims=True)
    shifted = values - center
    variance = jnp.mean(shifted * shifted, axis=-1, keepdims=True)
    return (shifted * lax.rsqrt(variance + EPS_LAYER) * gain_vec + bias_vec).astype(jnp.bfloat16)


def local(
    residual,
    wide_query,
    narrow_query,
    wide_keys,
    narrow_keys,
    wide_values,
    narrow_values,
    wide_query_gain,
    wide_key_gain,
    narrow_query_gain,
    narrow_key_gain,
    wide_out,
    narrow_out,
    first_gain,
    first_bias,
    route_ids,
    route_weights,
    expert_gate,
    expert_up,
    expert_down,
    shared_gate,
    shared_up,
    shared_down,
    second_gain,
    second_bias,
):
    tp_size = lax.axis_size("tp")
    out_weights = lax.all_gather(
        stacked(wide_out, narrow_out), "tp", axis=0, tiled=True
    )
    rotated_queries, own_pack = prepare(
        wide_query.T,
        narrow_query.T,
        wide_keys,
        narrow_keys,
        wide_values,
        narrow_values,
        wide_query_gain,
        wide_key_gain,
        narrow_query_gain,
        narrow_key_gain,
    )
    packs = [own_pack] + [turned_ring(own_pack, away) for away in range(1, SEQ_SHARDS)]
    earlier = attend(rotated_queries, packs[:2])
    mixed = attend(rotated_queries, packs[2:], earlier)
    tokens = lax.all_to_all(mixed, "tp", split_axis=0, concat_axis=1, tiled=True)
    projected = jnp.dot(tokens, out_weights, preferred_element_type=jnp.float32)
    hidden = layer_norm(ALPHA * residual.astype(jnp.float32) + projected, first_gain, first_bias)
    device_rows = hidden.shape[0]
    model_width = hidden.shape[1]
    sp_size = lax.axis_size("sp")
    top_count = route_ids.shape[1]
    experts = LOCAL_EXPERTS * sp_size
    capacity = max(2, (5 * device_rows * top_count + 4 * experts - 1) // (4 * experts))
    flat_ids = route_ids.reshape(-1)
    expert_hits = (flat_ids[:, None] == jnp.arange(experts, dtype=jnp.int32)[None, :]).astype(
        jnp.int32
    )
    earlier = jnp.sum((jnp.cumsum(expert_hits, axis=0) - expert_hits) * expert_hits, axis=1)
    slot_index = flat_ids * capacity + earlier
    chosen = (
        slot_index[:, None] == jnp.arange(experts * capacity, dtype=jnp.int32)[None, :]
    ).astype(jnp.float32)
    chosen = chosen.reshape(device_rows, top_count, experts * capacity)
    placing = jnp.sum(chosen, axis=1).astype(jnp.bfloat16)
    mixing = jnp.sum(chosen * route_weights[:, :, None], axis=1)
    outgoing = jnp.einsum("rs,rd->sd", placing, hidden, preferred_element_type=jnp.float32).astype(
        jnp.bfloat16
    )
    outgoing = outgoing.reshape(sp_size, LOCAL_EXPERTS, capacity, model_width)
    arrived = lax.all_to_all(outgoing, "sp", split_axis=0, concat_axis=0, tiled=True)
    slab = jnp.transpose(arrived, (1, 2, 0, 3)).reshape(
        LOCAL_EXPERTS, capacity * sp_size, model_width
    )
    core_lines = [list(range(core, tp_size, 2)) for core in range(2)]
    piece_rows = lax.all_gather(slab, "tp", axis=0, tiled=False, axis_index_groups=core_lines)
    gate_rows = jnp.transpose(expert_gate, (0, 2, 1))
    up_rows = jnp.transpose(expert_up, (0, 2, 1))
    partial_value = run_experts(
        piece_rows,
        gate_rows,
        other_core(gate_rows),
        up_rows,
        other_core(up_rows),
        expert_down,
        other_core(expert_down),
    )
    summed = lax.psum_scatter(
        partial_value, "tp", scatter_dimension=0, tiled=False, axis_index_groups=core_lines
    )
    summed = summed.reshape(LOCAL_EXPERTS, capacity, sp_size, model_width)
    returned = lax.all_to_all(
        jnp.transpose(summed, (2, 0, 1, 3)), "sp", split_axis=0, concat_axis=0, tiled=True
    )
    routed = jnp.dot(mixing, returned.reshape(-1, model_width).astype(jnp.float32))
    shared_gate_values = jnp.dot(hidden, shared_gate, preferred_element_type=jnp.float32)
    shared_up_values = jnp.dot(hidden, shared_up, preferred_element_type=jnp.float32)
    shared_active = (jax.nn.silu(shared_gate_values) * shared_up_values).astype(jnp.bfloat16)
    shared_output = jnp.dot(shared_active, shared_down, preferred_element_type=jnp.float32)
    base = lax.optimization_barrier(ALPHA * hidden.astype(jnp.float32) + shared_output)
    return layer_norm(base + routed, second_gain, second_bias)


def solution(mesh):
    in_specs = (
        P(("sp", "tp"), None),
        P("sp", "tp"),
        P("sp", "tp"),
        P("sp", None),
        P("sp", None),
        P("sp", None),
        P("sp", None),
        P(),
        P(),
        P(),
        P(),
        P("tp", None),
        P("tp", None),
        P(),
        P(),
        P(("sp", "tp"), None),
        P(("sp", "tp"), None),
        P("sp", None, "tp"),
        P("sp", None, "tp"),
        P("sp", "tp", None),
        P(),
        P(),
        P(),
        P(),
        P(),
    )
    out_specs = P(("sp", "tp"), None)
    return jax.shard_map(local, mesh=mesh, in_specs=in_specs, out_specs=out_specs, check_vma=False)
```
